512 devices in a mesh: sp: 128 (over z, y, core), tp: 4 (over x).
Axes of the slice: x: 4, y: 8, z: 8, core: 2. Of those that a mesh axis runs over, the one named last changes fastest.
Arguments:
- tokens: bfloat16 [65536, 2048], P('sp'), may hold values from -6 to 6
- norm_gain: float32 [2048], replicated, may hold values from 0.1 to 1.9
- w_value: bfloat16 [2048, 512], P('sp', 'tp'), may hold values from -0.125 to 0.125
- w_gate: bfloat16 [2048, 512], P('sp', 'tp'), may hold values from -0.125 to 0.125
- w_drive: bfloat16 [2048, 512], P('sp', 'tp'), may hold values from -0.125 to 0.125
- conv_taps: float32 [31, 512], P(None, 'tp'), may hold values from -12 to 12
- conv_gain: float32 [512], P('tp'), may hold values from 0.1 to 1.9
- log_step: float32 [32], P('tp'), may hold values from -20 to -3
- step_shift: float32 [65536, 32], P('sp', 'tp'), may hold values from -1.5 to 12
- state_real: float32 [32, 64], P('tp'), may hold values from -1.2 to -0.5
- state_imag: float32 [32, 64], P('tp'), may hold values from 0 to 201.06177
- in_map: float32 [2, 32, 64, 16], P(None, 'tp'), may hold values from -6 to 6
- out_map: float32 [2, 32, 16, 64], P(None, 'tp'), may hold values from -1.5 to 1.5
- skip_gain: float32 [32, 16], P('tp'), may hold values from -3 to 3
- start_state: float32 [2, 32, 64], P(None, 'tp'), may hold values from -6 to 6
- conv_proj: bfloat16 [512, 2048], P('tp', 'sp'), may hold values from -0.1875 to 0.1875
- state_proj: bfloat16 [512, 2048], P('tp', 'sp'), may hold values from -0.1875 to 0.1875
Outputs:
- mixed: bfloat16 [65536, 2048], P('sp', 'tp')
The draws below stay inside these ranges and needn't reach their ends.
All inputs are finite; a program needn't handle non-finite values.
Results may differ from the reference program's by a relative error of at most 0.013.
Values may be sent and summed in bfloat16 or wider, within the bound.
A program may use at most 64 MiB of HBM per device.

```python
import math
import jax
import jax.numpy as jnp
from jax import lax

D = 2048
CONV = 512
SSM = 512
GROUP = 16
STATE = 64
TAPS = 31
TOK_DEV = 512
GROUP_TOTAL = 32
TOKEN_LENGTH = 65536


def draw_conv_taps(key, part):
    first_key, second_key = jax.random.split(key)
    top_scale = 4.0
    rising = jnp.exp(math.log(top_scale) * jnp.arange(CONV, dtype=jnp.float32) / (CONV - 1))
    jitter = jnp.exp(jax.random.uniform(second_key, (CONV,), jnp.float32, -0.7, 0.7))
    normal_base = jnp.clip(jax.random.normal(first_key, (TAPS, CONV), jnp.float32), -4.0, 4.0)
    return normal_base * (rising * jitter / math.sqrt(TAPS))[None, :]


def draw_log_step(key, part):
    pick_key, jitter_key = jax.random.split(key)
    fast_share = 0.5
    fast_group = jax.random.bernoulli(pick_key, fast_share, (GROUP_TOTAL,))
    jitter = jax.random.uniform(jitter_key, (GROUP_TOTAL,), jnp.float32, -0.3, 0.3)
    slow_level = math.log(0.25 / TOKEN_LENGTH)
    fast_level = math.log(1.0 / 40.0)
    return jnp.where(fast_group, fast_level, slow_level) + jitter


def draw_step_shift(key, part):
    amplitude_key, coarse_key, location_key, spike_key = jax.random.split(key, 4)
    reach = 0.69
    block_count = TOKEN_LENGTH // TOK_DEV
    level = jax.random.uniform(amplitude_key, (block_count, 1, GROUP_TOTAL), jnp.float32, -reach, reach)
    rough = jax.random.uniform(coarse_key, (block_count, TOK_DEV, GROUP_TOTAL), jnp.float32, -0.35, 0.35)
    baseline_shift = (level + rough).reshape(TOKEN_LENGTH, GROUP_TOTAL)
    places = jax.random.randint(location_key, (3, GROUP_TOTAL), 0, TOKEN_LENGTH)
    spike_positions = jnp.any(jnp.arange(TOKEN_LENGTH)[:, None, None] == places[None], axis=1)
    spike_shift = math.log(1.5 * TOKEN_LENGTH) + jax.random.uniform(spike_key, (TOKEN_LENGTH, GROUP_TOTAL), jnp.float32, -0.3, 0.3)
    return jnp.where(spike_positions, spike_shift, baseline_shift)


def levels(stream_key, dims, cuts, low, high):
    def one(axis_at, shards_of):
        heights = jax.random.uniform(jax.random.fold_in(jax.random.fold_in(stream_key, 6), axis_at), (shards_of,), jnp.float32, low / len(cuts), high / len(cuts))
        return jnp.repeat(jnp.exp(heights), dims[axis_at] // shards_of).reshape((-1,) + (1,) * (len(dims) - axis_at - 1))

    level = one(*cuts[0])
    for cut in cuts[1:]:
        level = level * one(*cut)
    return level


def normal_values(rng, shape, scale, most, shards=(), kind=jnp.bfloat16):
    loudness = levels(rng, shape, shards, -0.22, 0.18) if shards else 1.0
    result = jax.random.normal(rng, shape, jnp.float32) * scale * loudness
    return jnp.minimum(jnp.maximum(result, -most), most).astype(kind)


def setup_inputs(seed: int = 0) -> dict:
    key_list = jax.random.split(jax.random.key(seed), 18)
    tokens = normal_values(key_list[0], (TOKEN_LENGTH, D), 1.0, 6.0, ((0, 128),))
    norm_gain = jnp.clip(1.0 + 0.18 * jax.random.normal(key_list[1], (D,), jnp.float32), 0.1, 1.9)
    w_value = normal_values(key_list[2], (D, CONV), D ** -0.5, 0.125, ((0, 128), (1, 4)))
    w_gate = normal_values(key_list[3], (D, CONV), D ** -0.5, 0.125, ((0, 128), (1, 4)))
    w_drive = normal_values(key_list[4], (D, SSM), D ** -0.5, 0.125, ((0, 128), (1, 4)))
    conv_taps = draw_conv_taps(jax.random.fold_in(key_list[17], 71), 0)
    conv_gain = jnp.clip(1.0 + 0.18 * jax.random.normal(key_list[6], (CONV,), jnp.float32), 0.1, 1.9)
    log_step = draw_log_step(jax.random.fold_in(key_list[17], 71), 0)
    step_shift = draw_step_shift(jax.random.fold_in(key_list[17], 71), 0)
    state_real = jnp.clip(-1.2 + 0.70000005 * jax.random.uniform(key_list[9], (GROUP_TOTAL, STATE), jnp.float32) ** levels(key_list[9], (GROUP_TOTAL, STATE), ((0, 4),), -0.2, 0.2), -1.2, -0.5)
    state_imag = jnp.clip(201.06177 * jax.random.uniform(key_list[10], (GROUP_TOTAL, STATE), jnp.float32) ** levels(key_list[10], (GROUP_TOTAL, STATE), ((0, 4),), -0.2, 0.2), 0.0, 201.06177)
    in_map = normal_values(key_list[11], (2, GROUP_TOTAL, STATE, GROUP), 1.0, 6.0, ((1, 4),), jnp.float32)
    out_map = normal_values(key_list[12], (2, GROUP_TOTAL, GROUP, STATE), 0.25, 1.5, ((1, 4),), jnp.float32)
    skip_gain = normal_values(key_list[13], (GROUP_TOTAL, GROUP), 0.5, 3.0, ((0, 4),), jnp.float32)
    start_state = normal_values(key_list[14], (2, GROUP_TOTAL, STATE), 1.0, 6.0, ((1, 4),), jnp.float32)
    conv_proj = normal_values(key_list[15], (CONV, D), (CONV + SSM) ** -0.5, 0.1875, ((0, 4), (1, 128)))
    state_proj = normal_values(key_list[16], (SSM, D), (CONV + SSM) ** -0.5, 0.1875, ((0, 4), (1, 128)))
    return dict(tokens=tokens, norm_gain=norm_gain, w_value=w_value, w_gate=w_gate, w_drive=w_drive, conv_taps=conv_taps, conv_gain=conv_gain, log_step=log_step, step_shift=step_shift, state_real=state_real, state_imag=state_imag, in_map=in_map, out_map=out_map, skip_gain=skip_gain, start_state=start_state, conv_proj=conv_proj, state_proj=state_proj)


def pair_combine(earlier, later):
    return (later[0] * earlier[0] - later[1] * earlier[1], later[0] * earlier[1] + later[1] * earlier[0], later[0] * earlier[2] - later[1] * earlier[3] + later[2], later[0] * earlier[3] + later[1] * earlier[2] + later[3])

def reference(tokens, norm_gain, w_value, w_gate, w_drive, conv_taps, conv_gain, log_step, step_shift, state_real, state_imag, in_map, out_map, skip_gain, start_state, conv_proj, state_proj):
    tokens_wide = tokens.astype(jnp.float32)
    inverse_rms = lax.rsqrt(lax.optimization_barrier(jnp.mean(tokens_wide * tokens_wide, axis=1, keepdims=True)) + 1e-06)
    normed = (tokens_wide * inverse_rms * norm_gain).astype(jnp.bfloat16)
    glu_value = jnp.dot(normed, w_value, preferred_element_type=jnp.float32).astype(jnp.bfloat16)
    glu_gate = jnp.dot(normed, w_gate, preferred_element_type=jnp.float32).astype(jnp.bfloat16)
    drive_in = jnp.dot(normed, w_drive, preferred_element_type=jnp.float32).astype(jnp.bfloat16)
    gated = (glu_value.astype(jnp.float32) * jax.nn.sigmoid(glu_gate.astype(jnp.float32))).astype(jnp.bfloat16)
    padded = jnp.concatenate([jnp.zeros((TAPS - 1, CONV), jnp.bfloat16), gated], axis=0)
    conv_mix = jnp.zeros((TOKEN_LENGTH, CONV), jnp.float32)
    for lag_index in range(TAPS):
        conv_mix = conv_mix + conv_taps[lag_index] * padded[lag_index:lag_index + TOKEN_LENGTH].astype(jnp.float32)
    row_mean = lax.optimization_barrier(jnp.mean(conv_mix, axis=1, keepdims=True))
    row_var = lax.optimization_barrier(jnp.mean(conv_mix * conv_mix, axis=1, keepdims=True)) - row_mean * row_mean
    conv_out = jax.nn.silu((conv_mix - row_mean) * lax.rsqrt(row_var + 1e-05) * conv_gain).astype(jnp.bfloat16)
    rate_re = state_real[None]
    rate_im = state_imag[None]
    rate_size = rate_re * rate_re + rate_im * rate_im
    block_count = TOKEN_LENGTH // TOK_DEV
    drive_blocks = drive_in.reshape(block_count, TOK_DEV, GROUP_TOTAL, GROUP)
    shift_blocks = step_shift.reshape(block_count, TOK_DEV, GROUP_TOTAL)

    def sweep(state_carry, inputs):
        carry_re, carry_im = state_carry
        drive_block, shift_block = inputs
        drive_wide = drive_block.astype(jnp.float32)
        step_full = jnp.exp(log_step[None, :] + shift_block)[:, :, None]
        decay_mag = jnp.exp(rate_re * step_full)
        keep_re = decay_mag * jnp.cos(rate_im * step_full)
        keep_im = decay_mag * jnp.sin(rate_im * step_full)
        mapped_re = jnp.einsum('tgh,gph->tgp', drive_wide, in_map[0], precision=lax.Precision.HIGHEST)
        mapped_im = jnp.einsum('tgh,gph->tgp', drive_wide, in_map[1], precision=lax.Precision.HIGHEST)
        minus_re = keep_re - 1.0
        coeff_re = (minus_re * rate_re + keep_im * rate_im) / rate_size
        coeff_im = (keep_im * rate_re - minus_re * rate_im) / rate_size
        input_re = coeff_re * mapped_re - coeff_im * mapped_im
        input_im = coeff_re * mapped_im + coeff_im * mapped_re
        cum_re, cum_im, local_re, local_im = lax.associative_scan(pair_combine, (keep_re, keep_im, input_re, input_im), axis=0)
        state_re = local_re + cum_re * carry_re[None] - cum_im * carry_im[None]
        state_im = local_im + cum_re * carry_im[None] + cum_im * carry_re[None]
        ssm_pre = jnp.einsum('tgp,ghp->tgh', state_re, out_map[0], precision=lax.Precision.HIGHEST) - jnp.einsum('tgp,ghp->tgh', state_im, out_map[1], precision=lax.Precision.HIGHEST) + skip_gain * drive_wide
        block_out = jax.nn.gelu(ssm_pre).reshape(TOK_DEV, SSM).astype(jnp.bfloat16)
        return ((state_re[-1], state_im[-1]), block_out)
    carried, ssm_blocks = lax.scan(sweep, (start_state[0], start_state[1]), (drive_blocks, shift_blocks))
    ssm_out = ssm_blocks.reshape(TOKEN_LENGTH, SSM)
    mixed = jnp.dot(conv_out, conv_proj, preferred_element_type=jnp.float32) + jnp.dot(ssm_out, state_proj, preferred_element_type=jnp.float32)
    return mixed.astype(jnp.bfloat16)
```

```python
import functools
import math

import jax
import jax.numpy as jnp
from jax import lax
from jax.experimental import pallas as pl
from jax.experimental.pallas import tpu as pltpu
from jax.sharding import PartitionSpec as P

MESH = pl.DeviceIdType.MESH
F32, BF16 = jnp.float32, jnp.bfloat16
HIGHEST = lax.Precision.HIGHEST
CHUNKS = 8
LANES = 128
PI_HEAD, PI_MID, PI_TAIL = 3.140625, 9.67502593994140625e-4, 1.509957990978376432e-7
SIN = (
    0.9999999956945582,
    -0.16666657935421791,
    0.008333049779224343,
    -0.00019808982983932522,
    2.605019582042587e-06,
)
COS = (
    0.9999999997785899,
    -0.4999999935376166,
    0.04166663608814349,
    -0.0013888359276841241,
    2.476005397141232e-05,
    -2.6049608226484117e-07,
)


def series(terms, x):
    total = terms[-1]
    for term in reversed(terms[:-1]):
        total = total * x + term
    return total


def keep_of(rate_re, rate_im, step):
    angle = rate_im * step
    turns = jnp.floor(angle * (1.0 / math.pi) + 0.5)
    rest = ((angle - turns * PI_HEAD) - turns * PI_MID) - turns * PI_TAIL
    square = rest * rest
    half = turns * 0.5
    size = jnp.exp(rate_re * step) * (1.0 - 4.0 * (half - jnp.floor(half)))
    return size * series(COS, square), size * (rest * series(SIN, square))


def nn(a, b, precision=None):
    return lax.dot_general(
        a, b, (((1,), (0,)), ((), ())), precision=precision, preferred_element_type=F32
    )


def nt(a, b, precision=None):
    return lax.dot_general(
        a, b, (((1,), (1,)), ((), ())), precision=precision, preferred_element_type=F32
    )


def tn(a, b, precision=None):
    return lax.dot_general(
        a, b, (((0,), (0,)), ((), ())), precision=precision, preferred_element_type=F32
    )


def ids(shape, dim):
    return lax.broadcasted_iota(jnp.int32, shape, dim)


def split_two(x):
    head = x.astype(BF16)
    return head, (x - head.astype(F32)).astype(BF16)


def entry_of(arrived, side, place, rate_re, rate_im, q):
    real = arrived[pl.ds(q, side, stride=16), :]
    imag = arrived[pl.ds(4 + q, side, stride=16), :]
    step = arrived[pl.ds(8 + q, side, stride=16), :]
    row = ids((side, LANES), 0)
    since = jnp.zeros((side, LANES), F32)
    for k in range(side):
        since = since + jnp.where((row < k) & (place > k), step[k : k + 1], 0.0)
    turn_re, turn_im = keep_of(rate_re, rate_im, since)
    before = row < place
    got_re = jnp.where(before, turn_re * real - turn_im * imag, 0.0)
    got_im = jnp.where(before, turn_re * imag + turn_im * real, 0.0)
    ahead = jnp.where(before, step, 0.0)
    return (
        jnp.sum(got_re, axis=0, keepdims=True),
        jnp.sum(got_im, axis=0, keepdims=True),
        jnp.sum(ahead, axis=0, keepdims=True),
    )


def kernel(
    dims,
    tokens_hbm,
    value_hbm,
    gate_hbm,
    drive_hbm,
    convp_hbm,
    statep_hbm,
    gain_ref,
    taps_ref,
    conv_gain_ref,
    log_step_ref,
    shift_ref,
    rate_re_ref,
    rate_im_ref,
    in_ref,
    out_map_ref,
    skip_ref,
    start_ref,
    out_ref,
    tok,
    nrm,
    gd,
    gv,
    pz,
    py,
    wd,
    wvg,
    wo,
    dtx,
    kr,
    ki,
    cr,
    ci,
    mr,
    mi,
    in_blocks,
    out_blocks,
    drv,
    drvp,
    gf,
    cm,
    halo,
    halo_send,
    st_send,
    st_recv,
    mc_send,
    mc_recv,
    my_all,
    mz_all,
    act,
    local_sem,
    d1s,
    d1r,
    v1s,
    v1r,
    p1s,
    p1r,
    d2s,
    d2r,
    v2s,
    v2r,
    p2s,
    p2r,
    p3s,
    p3r,
    dcs,
    dcr,
    vcs,
    vcr,
    pcs,
    pcr,
    misc_s,
    misc_r,
    cys,
    cyr,
    czs,
    czr,
    sts,
    strv,
    acs,
    acr,
    ass,
    asr,
):
    side, cols = dims
    rows, depth = tokens_hbm.shape
    planes = side // cols
    sp, x = lax.axis_index("sp"), lax.axis_index("tp")
    c = lax.rem(sp, 2)
    chip = lax.div(sp, 2)
    y, z = lax.rem(chip, side), lax.div(chip, side)
    count = 2 * side * side
    steps = rows // CHUNKS

    def at(zz, yy, cc):
        return (zz * side + yy) * 2 + cc

    def turn(a, k):
        return lax.rem(a + k, side)

    mate = at(z, y, 1 - c)
    b_me, a_me = c * z + (1 - c) * y, c * y + (1 - c) * z

    def b_peer(b):
        return c * at(b, y, 1) + (1 - c) * at(z, b, 0)

    def a_peer(a):
        return c * at(z, a, 1) + (1 - c) * at(a, y, 0)

    beyond = lax.rem(sp + 2 * c - 1 + count, count)
    following = lax.rem(sp + 1, count)

    def copy(src, dst, send_sem, recv_sem, to_sp, to_x):
        return pltpu.make_async_remote_copy(
            src_ref=src,
            dst_ref=dst,
            send_sem=send_sem,
            recv_sem=recv_sem,
            device_id=(to_sp, to_x),
            device_id_type=MESH,
        )

    sent = []

    def send(*args):
        one = copy(*args)
        one.start()
        sent.append(one)

    def arrive(dst, send_sem, recv_sem):
        copy(dst, dst, send_sem, recv_sem, mate, x).wait_recv()

    own_copies = [
        pltpu.make_async_copy(drive_hbm, gd.at[c, a_me, b_me], local_sem.at[0]),
        pltpu.make_async_copy(value_hbm, gv.at[c, a_me, b_me, :, pl.ds(0, LANES)], local_sem.at[1]),
        pltpu.make_async_copy(gate_hbm, gv.at[c, a_me, b_me, :, pl.ds(LANES, LANES)], local_sem.at[2]),
        pltpu.make_async_copy(convp_hbm, pz.at[z, :, pl.ds(0, LANES)], local_sem.at[3]),
        pltpu.make_async_copy(statep_hbm, pz.at[z, :, pl.ds(LANES, LANES)], local_sem.at[4]),
        pltpu.make_async_copy(tokens_hbm, tok, local_sem.at[5]),
    ]
    for one in own_copies:
        one.start()

    barrier = pltpu.get_barrier_semaphore()

    def greet(to_sp, to_x):
        pl.semaphore_signal(barrier, inc=1, device_id=(to_sp, to_x), device_id_type=MESH)

    greet(mate, x)
    greet(beyond, x)
    for k in range(1, side):
        greet(at(z, turn(y, k), c), x)
        greet(at(turn(z, k), y, c), x)
    for k in range(1, cols):
        greet(sp, lax.rem(x + k, cols))

    wide = 4 * LANES
    group_mask = (ids((LANES, wide), 1) // 64 == ids((LANES, wide), 0) // 16).astype(F32)
    spread = (ids((64, wide), 1) % 64 == ids((64, wide), 0)).astype(F32)
    for half in range(2):
        part = pl.ds(half * LANES, LANES)
        tiled = nn(in_ref[part, :], spread, HIGHEST) * group_mask
        head, tail = split_two(tiled)
        in_blocks[half, 0], in_blocks[half, 1] = head, tail
        tiled = nn(out_map_ref[part, :], spread, HIGHEST) * group_mask
        head, tail = split_two(tiled)
        out_blocks[half, 0], out_blocks[half, 1] = head, tail
    own_group = (ids((8, wide), 1) // 64 == ids((8, wide), 0)).astype(F32)

    def flat(value):
        return jnp.sum(nn(value, spread, HIGHEST) * own_group, axis=0, keepdims=True)

    rate_re, rate_im = flat(rate_re_ref[...]), flat(rate_im_ref[...])
    first_re, first_im = flat(start_ref[0:8, :]), flat(start_ref[8:16, :])
    size = rate_re * rate_re + rate_im * rate_im
    inv_re, inv_im = rate_re / size, rate_im / size
    spread16 = (ids((16, LANES), 1) % 16 == ids((16, LANES), 0)).astype(F32)
    own16 = (ids((8, LANES), 1) // 16 == ids((8, LANES), 0)).astype(F32)
    skip_row = jnp.sum(nn(skip_ref[...], spread16, HIGHEST) * own16, axis=0, keepdims=True)
    eye8 = ids((8, 8), 0) == ids((8, 8), 1)
    log_step = jnp.sum(jnp.where(eye8, log_step_ref[...], 0.0), axis=1, keepdims=True)
    dt = jnp.exp(log_step + shift_ref[...])

    def tile(v, q):
        return v[:, q * LANES : (q + 1) * LANES]

    for q in range(4):
        dtx[q] = tn(dt, tile(own_group, q), HIGHEST)

    pl.semaphore_wait(barrier, 2 * side + cols - 1)
    for one in own_copies[:5]:
        one.wait()
    for k in range(1, side):
        here = gd.at[c, a_me, b_me]
        send(here, here, d1s.at[k], d1r.at[k], b_peer(turn(b_me, k)), x)
    for k in range(1, side):
        here = gv.at[c, a_me, b_me]
        send(here, here, v1s.at[k], v1r.at[k], b_peer(turn(b_me, k)), x)
    for k in range(1, side):
        here = pz.at[z]
        send(here, here, p1s.at[k], p1r.at[k], at(turn(z, k), y, c), x)

    own_copies[5].wait()
    gain = gain_ref[...]

    def norm_rows(i, carry):
        r = pl.ds(pl.multiple_of(i * 16, 16), 16)
        wide_rows = tok[r, :].astype(F32)
        mean = jnp.sum(wide_rows * wide_rows, axis=1, keepdims=True) * (1.0 / depth)
        nrm[r, :] = (wide_rows * lax.rsqrt(mean + 1e-06) * gain).astype(BF16)
        return carry

    lax.fori_loop(0, rows // 16, norm_rows, 0)

    for k in range(1, side):
        arrive(gd.at[c, a_me, turn(b_me, side - k)], d1s.at[k], d1r.at[k])
    line = gd.at[c, a_me]
    for k in range(1, side):
        send(line, line, d2s.at[k], d2r.at[k], a_peer(turn(a_me, k)), x)
    send(line, line, dcs.at[0], dcr.at[0], mate, x)
    for k in range(1, side):
        arrive(gv.at[c, a_me, turn(b_me, side - k)], v1s.at[k], v1r.at[k])
    line = gv.at[c, a_me]
    for k in range(1, side):
        send(line, line, v2s.at[k], v2r.at[k], a_peer(turn(a_me, k)), x)
    send(line, line, vcs.at[0], vcr.at[0], mate, x)
    for k in range(1, side):
        arrive(pz.at[turn(z, side - k)], p1s.at[k], p1r.at[k])
    for k in range(1, cols):
        to = lax.rem(x + k, cols)
        send(pz.at[pl.ds(to * planes, planes)], py.at[c, y, x], p2s.at[k], p2r.at[k], sp, to)
    py[c, y, x] = pz[pl.ds(x * planes, planes)]

    def keep_rows(j, carry):
        r = pl.ds(pl.multiple_of(j * 8, 8), 8)
        new = []
        for q in range(4):
            step = dtx[q, pl.ds(j, CHUNKS, stride=steps), :]
            keep_re, keep_im = keep_of(tile(rate_re, q), tile(rate_im, q), step)
            minus = keep_re - 1.0
            cols_q = pl.ds(q * LANES, LANES)
            kr[r, cols_q] = keep_re
            ki[r, cols_q] = keep_im
            cr[r, cols_q] = minus * tile(inv_re, q) + keep_im * tile(inv_im, q)
            ci[r, cols_q] = keep_im * tile(inv_re, q) - minus * tile(inv_im, q)
            new.append(carry[q] + step)
        return tuple(new)

    zero = jnp.zeros((CHUNKS, LANES), F32)
    spans = lax.fori_loop(0, steps, keep_rows, (zero,) * 4)

    for k in range(1, side):
        block = gd.at[c, turn(a_me, side - k)]
        arrive(block, d2s.at[k], d2r.at[k])
        send(block, block, dcs.at[k], dcr.at[k], mate, x)
    for k in range(side):
        arrive(gd.at[1 - c, turn(b_me, side - k)], dcs.at[k], dcr.at[k])

    def place_drive(a, carry):
        for b in range(side):
            r = pl.multiple_of(at(a, b, 0) * 16, 16)
            wd[pl.ds(r, 16), :] = gd[0, a, b]
            r = pl.multiple_of(at(b, a, 1) * 16, 16)
            wd[pl.ds(r, 16), :] = gd[1, a, b]
        return carry

    lax.fori_loop(0, side, place_drive, 0)
    block_rows = min(rows, 128)

    def drive_rows(i, carry):
        r = pl.ds(pl.multiple_of(i * block_rows, block_rows), block_rows)
        drv[r, :] = nn(nrm[r, :], wd[...]).astype(BF16).astype(F32)
        return carry

    lax.fori_loop(0, rows // block_rows, drive_rows, 0)

    def turn_rows(j, carry):
        r = pl.ds(pl.multiple_of(j * 8, 8), 8)
        drvp[r, :] = drv[pl.ds(j, CHUNKS, stride=steps), :]
        return carry

    lax.fori_loop(0, steps, turn_rows, 0)

    def map_rows(i, carry):
        r = pl.ds(pl.multiple_of(i * block_rows, block_rows), block_rows)
        d = drvp[r, :].astype(BF16)
        mr[r, :] = nn(d, in_blocks[0, 0]) + nn(d, in_blocks[0, 1])
        mi[r, :] = nn(d, in_blocks[1, 0]) + nn(d, in_blocks[1, 1])
        return carry

    lax.fori_loop(0, rows // block_rows, map_rows, 0)

    def scan_rows(j, carry):
        r = pl.ds(pl.multiple_of(j * 8, 8), 8)
        new = []
        for q in range(4):
            cols_q = pl.ds(q * LANES, LANES)
            s_re, s_im = carry[2 * q], carry[2 * q + 1]
            c_re, c_im = cr[r, cols_q], ci[r, cols_q]
            m_re, m_im = mr[r, cols_q], mi[r, cols_q]
            u_re = c_re * m_re - c_im * m_im
            u_im = c_re * m_im + c_im * m_re
            cr[r, cols_q] = u_re
            ci[r, cols_q] = u_im
            k_re, k_im = kr[r, cols_q], ki[r, cols_q]
            new.append((k_re * s_re + u_re) - k_im * s_im)
            new.append((k_re * s_im + u_im) + k_im * s_re)
        return tuple(new)

    finals = lax.fori_loop(0, steps, scan_rows, (zero,) * 8)

    row8 = ids((CHUNKS, LANES), 0)
    starts, mine, ahead_spans = [], [], []
    for q in range(4):
        re_q, im_q = tile(rate_re, q), tile(rate_im, q)
        hop_re, hop_im = keep_of(re_q, im_q, spans[q])
        f_re, f_im = finals[2 * q], finals[2 * q + 1]
        e_re = e_im = total = jnp.zeros((1, LANES), F32)
        l_re = l_im = ahead = zero
        for s in range(CHUNKS):
            l_re = jnp.where(row8 == s, e_re, l_re)
            l_im = jnp.where(row8 == s, e_im, l_im)
            ahead = jnp.where(row8 == s, total, ahead)
            h_re, h_im = hop_re[s : s + 1], hop_im[s : s + 1]
            e_re, e_im = (
                h_re * e_re - h_im * e_im + f_re[s : s + 1],
                h_re * e_im + h_im * e_re + f_im[s : s + 1],
            )
            total = total + spans[q][s : s + 1]
        starts.append((l_re, l_im))
        ahead_spans.append(ahead)
        mine.append((e_re, e_im, total))
        mc_send[q : q + 1, :] = e_re
        mc_send[4 + q : 5 + q, :] = e_im
        mc_send[8 + q : 9 + q, :] = total
    mc_send[12:16, :] = jnp.zeros((4, LANES), F32)
    send(mc_send, mc_recv, misc_s.at[0], misc_r.at[0], mate, x)

    for k in range(1, side):
        block = gv.at[c, turn(a_me, side - k)]
        arrive(block, v2s.at[k], v2r.at[k])
        send(block, block, vcs.at[k], vcr.at[k], mate, x)

    arrive(mc_recv, misc_s.at[0], misc_r.at[0])
    core_entry = []
    second = c == 1
    slot = pl.multiple_of(y * 16, 16)
    for q in range(4):
        re_q, im_q = tile(rate_re, q), tile(rate_im, q)
        m_re, m_im, m_span = mine[q]
        o_re, o_im = mc_recv[q : q + 1, :], mc_recv[4 + q : 5 + q, :]
        o_span = mc_recv[8 + q : 9 + q, :]
        a_re, a_im = jnp.where(second, o_re, m_re), jnp.where(second, o_im, m_im)
        b_re, b_im = jnp.where(second, m_re, o_re), jnp.where(second, m_im, o_im)
        h_re, h_im = keep_of(re_q, im_q, jnp.where(second, m_span, o_span))
        my_all[pl.ds(slot + q, 1), :] = h_re * a_re - h_im * a_im + b_re
        my_all[pl.ds(slot + 4 + q, 1), :] = h_re * a_im + h_im * a_re + b_im
        my_all[pl.ds(slot + 8 + q, 1), :] = m_span + o_span
        none = jnp.zeros_like(o_re)
        core_entry.append(
            (
                jnp.where(second, o_re, none),
                jnp.where(second, o_im, none),
                jnp.where(second, o_span, none),
            )
        )
    my_all[pl.ds(slot + 12, 4), :] = jnp.zeros((4, LANES), F32)
    here = my_all.at[pl.ds(slot, 16), :]
    for k in range(1, side):
        send(here, here, cys.at[k], cyr.at[k], at(z, turn(y, k), c), x)

    for k in range(side):
        arrive(gv.at[1 - c, turn(b_me, side - k)], vcs.at[k], vcr.at[k])

    def place_value(a, carry):
        for b in range(side):
            r = pl.multiple_of(at(a, b, 0) * 16, 16)
            wvg[pl.ds(r, 16), :] = gv[0, a, b]
            r = pl.multiple_of(at(b, a, 1) * 16, 16)
            wvg[pl.ds(r, 16), :] = gv[1, a, b]
        return carry

    lax.fori_loop(0, side, place_value, 0)

    def gate_rows(i, carry):
        i = rows // block_rows - 1 - i
        base = pl.multiple_of(i * block_rows, block_rows)
        both = nn(nrm[pl.ds(base, block_rows), :], wvg[...]).astype(BF16).astype(F32)
        gated = (both[:, :LANES] * jax.nn.sigmoid(both[:, LANES:])).astype(BF16)
        gf[pl.ds(base + 32, block_rows), :] = gated.astype(F32)
        return carry

    lax.fori_loop(0, rows // block_rows, gate_rows, 0)
    halo_send[...] = gf[rows : rows + 32, :].astype(BF16)
    send(halo_send, halo, misc_s.at[1], misc_r.at[1], following, x)

    for k in range(1, side):
        from_y = turn(y, side - k)
        arrive(my_all.at[pl.ds(pl.multiple_of(from_y * 16, 16), 16), :], cys.at[k], cyr.at[k])
    chip_entry = []
    slot_z = pl.multiple_of(z * 16, 16)
    for q in range(4):
        re_q, im_q = tile(rate_re, q), tile(rate_im, q)
        chip_entry.append(entry_of(my_all, side, y, re_q, im_q, q))
        all_re, all_im, all_span = entry_of(my_all, side, side, re_q, im_q, q)
        mz_all[pl.ds(slot_z + q, 1), :] = all_re
        mz_all[pl.ds(slot_z + 4 + q, 1), :] = all_im
        mz_all[pl.ds(slot_z + 8 + q, 1), :] = all_span
    mz_all[pl.ds(slot_z + 12, 4), :] = jnp.zeros((4, LANES), F32)
    here = mz_all.at[pl.ds(slot_z, 16), :]
    for k in range(1, side):
        send(here, here, czs.at[k], czr.at[k], at(turn(z, k), y, c), x)

    arrive(halo, misc_s.at[1], misc_r.at[1])
    gf[0:32, :] = jnp.where(sp == 0, 0.0, halo[...].astype(F32))
    taps = taps_ref.shape[0]
    conv_rows = min(rows, 64)

    def conv_block(i, carry):
        base = pl.multiple_of(i * conv_rows, conv_rows)
        total = jnp.zeros((conv_rows, LANES), F32)
        for k in range(taps):
            total = total + taps_ref[k : k + 1, :] * gf[pl.ds(base + (33 - taps) + k, conv_rows), :]
        cm[pl.ds(base, conv_rows), :] = total
        return carry

    lax.fori_loop(0, rows // conv_rows, conv_block, 0)
    mix = cm[...]
    ones = jnp.ones((8, LANES), F32)
    row_st = ids((8, rows), 0)
    sums = nt(ones, mix, HIGHEST)
    squares = nt(ones, mix * mix, HIGHEST)
    st_send[...] = jnp.where(row_st == 0, sums, jnp.where(row_st == 1, squares, 0.0))
    for k in range(1, cols):
        send(st_send, st_recv.at[k - 1], sts.at[k], strv.at[k], sp, lax.rem(x + k, cols))

    for k in range(1, cols):
        arrive(py.at[c, y, lax.rem(x + cols - k, cols)], p2s.at[k], p2r.at[k])
    line = py.at[c, y]
    for k in range(1, side):
        send(line, line, p3s.at[k], p3r.at[k], at(z, turn(y, k), c), x)
    send(line, line, pcs.at[0], pcr.at[0], mate, x)

    stats = st_send[...]
    for k in range(1, cols):
        arrive(st_recv.at[k - 1], sts.at[k], strv.at[k])
        stats = stats + st_recv[k - 1]
    stats = stats * (1.0 / (cols * LANES))
    pick = ids((8, LANES), 0)
    mean = tn(stats, (pick == 0).astype(F32), HIGHEST)
    square = tn(stats, (pick == 1).astype(F32), HIGHEST)
    scaled = (cm[...] - mean) * lax.rsqrt(square - mean * mean + 1e-05) * conv_gain_ref[...]
    act[x, :, pl.ds(0, LANES)] = (scaled * jax.nn.sigmoid(scaled)).astype(BF16)
    here = act.at[x, :, pl.ds(0, LANES)]
    for k in range(1, cols):
        send(here, here, acs.at[k], acr.at[k], sp, lax.rem(x + k, cols))

    for k in range(1, side):
        from_z = turn(z, side - k)
        arrive(mz_all.at[pl.ds(pl.multiple_of(from_z * 16, 16), 16), :], czs.at[k], czr.at[k])
    begin = []
    for q in range(4):
        re_q, im_q = tile(rate_re, q), tile(rate_im, q)
        s_re, s_im = tile(first_re, q), tile(first_im, q)
        for more_re, more_im, span in (
            entry_of(mz_all, side, z, re_q, im_q, q),
            chip_entry[q],
            core_entry[q],
        ):
            h_re, h_im = keep_of(re_q, im_q, span)
            s_re, s_im = h_re * s_re - h_im * s_im + more_re, h_re * s_im + h_im * s_re + more_im
        h_re, h_im = keep_of(re_q, im_q, ahead_spans[q])
        begin.append(h_re * s_re - h_im * s_im + starts[q][0])
        begin.append(h_re * s_im + h_im * s_re + starts[q][1])

    def state_rows(j, carry):
        r = pl.ds(pl.multiple_of(j * 8, 8), 8)
        new = []
        for q in range(4):
            cols_q = pl.ds(q * LANES, LANES)
            s_re, s_im = carry[2 * q], carry[2 * q + 1]
            k_re, k_im = kr[r, cols_q], ki[r, cols_q]
            n_re = (k_re * s_re + cr[r, cols_q]) - k_im * s_im
            n_im = (k_re * s_im + ci[r, cols_q]) + k_im * s_re
            mr[r, cols_q] = n_re
            mi[r, cols_q] = n_im
            new.extend((n_re, n_im))
        return tuple(new)

    lax.fori_loop(0, steps, state_rows, tuple(begin))

    def read_rows(i, carry):
        r = pl.ds(pl.multiple_of(i * block_rows, block_rows), block_rows)
        re_head, re_tail = split_two(mr[r, :])
        im_head, im_tail = split_two(mi[r, :])
        total = nt(re_head, out_blocks[0, 0]) - nt(im_head, out_blocks[1, 0])
        total = total + (nt(re_tail, out_blocks[0, 0]) - nt(im_tail, out_blocks[1, 0]))
        total = total + (nt(re_head, out_blocks[0, 1]) - nt(im_head, out_blocks[1, 1]))
        drvp[r, :] = jax.nn.gelu(total + skip_row * drvp[r, :])
        return carry

    lax.fori_loop(0, rows // block_rows, read_rows, 0)

    def back_rows(j, carry):
        r = pl.ds(pl.multiple_of(j * 8, 8), 8)
        drv[pl.ds(j, CHUNKS, stride=steps), :] = drvp[r, :]
        return carry

    lax.fori_loop(0, steps, back_rows, 0)
    act[x, :, pl.ds(LANES, LANES)] = drv[...].astype(BF16)
    here = act.at[x, :, pl.ds(LANES, LANES)]
    for k in range(1, cols):
        send(here, here, ass.at[k], asr.at[k], sp, lax.rem(x + k, cols))

    for k in range(1, side):
        block = py.at[c, turn(y, side - k)]
        arrive(block, p3s.at[k], p3r.at[k])
        send(block, block, pcs.at[k], pcr.at[k], mate, x)
    for k in range(side):
        arrive(py.at[1 - c, turn(y, side - k)], pcs.at[k], pcr.at[k])

    def place_out(b, carry):
        for core in range(2):
            for col in range(cols):
                for plane in range(planes):
                    r = pl.multiple_of((plane * side + b) * 32 + core * 16, 16)
                    wo[col, pl.ds(r, 16), :] = py[core, b, col, plane]
        return carry

    lax.fori_loop(0, side, place_out, 0)
    for k in range(1, cols):
        from_x = lax.rem(x + cols - k, cols)
        arrive(act.at[from_x, :, pl.ds(0, LANES)], acs.at[k], acr.at[k])
        arrive(act.at[from_x, :, pl.ds(LANES, LANES)], ass.at[k], asr.at[k])

    def out_rows(i, carry):
        r = pl.ds(pl.multiple_of(i * block_rows, block_rows), block_rows)
        total = nt(act[0, r, :], wo[0])
        for col in range(1, cols):
            total = total + nt(act[col, r, :], wo[col])
        out_ref[r, :] = total.astype(BF16)
        return carry

    lax.fori_loop(0, rows // block_rows, out_rows, 0)
    for one in sent:
        one.wait_send()


def on_device(
    side,
    cols,
    tokens,
    norm_gain,
    w_value,
    w_gate,
    w_drive,
    conv_taps,
    conv_gain,
    log_step,
    step_shift,
    state_real,
    state_imag,
    in_map,
    out_map,
    skip_gain,
    start_state,
    conv_proj,
    state_proj,
):
    rows, depth = tokens.shape
    planes = side // cols
    out_cols = planes * side * 32
    groups, states = state_real.shape
    width = groups * states
    hbm = pl.BlockSpec(memory_space=pltpu.HBM)
    vmem = pl.BlockSpec(memory_space=pltpu.VMEM)
    dma = pltpu.SemaphoreType.DMA
    near, line = dma((cols,)), dma((side,))
    return pl.pallas_call(
        functools.partial(kernel, (side, cols)),
        out_shape=jax.ShapeDtypeStruct((rows, out_cols), BF16),
        in_specs=[hbm] * 6 + [vmem] * 11,
        out_specs=vmem,
        scratch_shapes=[
            pltpu.VMEM((rows, depth), BF16),
            pltpu.VMEM((rows, depth), BF16),
            pltpu.VMEM((2, side, side, 16, LANES), BF16),
            pltpu.VMEM((2, side, side, 16, 2 * LANES), BF16),
            pltpu.VMEM((side, 16, 2 * LANES), BF16),
            pltpu.VMEM((2, side, cols, planes, 16, 2 * LANES), BF16),
            pltpu.VMEM((depth, LANES), BF16),
            pltpu.VMEM((depth, 2 * LANES), BF16),
            pltpu.VMEM((cols, out_cols, 2 * LANES), BF16),
            pltpu.VMEM((4, rows, LANES), F32),
            *[pltpu.VMEM((rows, width), F32)] * 6,
            pltpu.VMEM((2, 2, LANES, width), BF16),
            pltpu.VMEM((2, 2, LANES, width), BF16),
            pltpu.VMEM((rows, LANES), F32),
            pltpu.VMEM((rows, LANES), F32),
            pltpu.VMEM((rows + 32, LANES), F32),
            pltpu.VMEM((rows, LANES), F32),
            pltpu.VMEM((32, LANES), BF16),
            pltpu.VMEM((32, LANES), BF16),
            pltpu.VMEM((8, rows), F32),
            pltpu.VMEM((cols - 1, 8, rows), F32),
            pltpu.VMEM((16, LANES), F32),
            pltpu.VMEM((16, LANES), F32),
            pltpu.VMEM((side * 16, LANES), F32),
            pltpu.VMEM((side * 16, LANES), F32),
            pltpu.VMEM((cols, rows, 2 * LANES), BF16),
            dma((6,)),
            *[line] * 10,
            near,
            near,
            line,
            line,
            *[line] * 6,
            dma((2,)),
            dma((2,)),
            *[line] * 4,
            *[near] * 6,
        ],
        compiler_params=pltpu.CompilerParams(
            collective_id=0, has_side_effects=True, vmem_limit_bytes=60 * 1024 * 1024
        ),
    )(
        tokens,
        w_value,
        w_gate,
        w_drive,
        conv_proj.T,
        state_proj.T,
        norm_gain.reshape(1, depth),
        conv_taps,
        conv_gain.reshape(1, -1),
        log_step.reshape(1, -1),
        step_shift.T,
        state_real,
        state_imag,
        jnp.transpose(in_map, (0, 1, 3, 2)).reshape(-1, states),
        out_map.reshape(-1, states),
        skip_gain,
        start_state.reshape(-1, states),
    )


def solution(mesh):
    side = math.isqrt(mesh.shape["sp"] // 2)
    placed = (
        P("sp", None),
        P(),
        P("sp", "tp"),
        P("sp", "tp"),
        P("sp", "tp"),
        P(None, "tp"),
        P("tp"),
        P("tp"),
        P("sp", "tp"),
        P("tp", None),
        P("tp", None),
        P(None, "tp", None, None),
        P(None, "tp", None, None),
        P("tp", None),
        P(None, "tp", None),
        P("tp", "sp"),
        P("tp", "sp"),
    )
    return jax.shard_map(
        functools.partial(on_device, side, mesh.shape["tp"]),
        mesh=mesh,
        in_specs=placed,
        out_specs=P("sp", "tp"),
        check_vma=False,
    )
```

```python
import functools
import math

import jax
import jax.numpy as jnp
from jax import lax
from jax.experimental import pallas as pl
from jax.experimental.pallas import tpu as pltpu
from jax.sharding import PartitionSpec as P

MESH = pl.DeviceIdType.MESH
F32, BF16 = jnp.float32, jnp.bfloat16
HIGHEST = lax.Precision.HIGHEST
CHUNKS = 8
LANES = 128
PI_HEAD, PI_MID, PI_TAIL = 3.140625, 9.67502593994140625e-4, 1.509957990978376432e-7
SIN = (
    0.9999999956945582,
    -0.16666657935421791,
    0.008333049779224343,
    -0.00019808982983932522,
    2.605019582042587e-06,
)
COS = (
    0.9999999997785899,
    -0.4999999935376166,
    0.04166663608814349,
    -0.0013888359276841241,
    2.476005397141232e-05,
    -2.6049608226484117e-07,
)


def series(terms, x):
    total = terms[-1]
    for term in reversed(terms[:-1]):
        total = total * x + term
    return total


def keep_of(rate_re, rate_im, step):
    angle = rate_im * step
    turns = jnp.floor(angle * (1.0 / math.pi) + 0.5)
    rest = ((angle - turns * PI_HEAD) - turns * PI_MID) - turns * PI_TAIL
    square = rest * rest
    half = turns * 0.5
    size = jnp.exp(rate_re * step) * (1.0 - 4.0 * (half - jnp.floor(half)))
    return size * series(COS, square), size * (rest * series(SIN, square))


def nn(a, b, precision=None):
    return lax.dot_general(
        a, b, (((1,), (0,)), ((), ())), precision=precision, preferred_element_type=F32
    )


def nt(a, b, precision=None):
    return lax.dot_general(
        a, b, (((1,), (1,)), ((), ())), precision=precision, preferred_element_type=F32
    )


def tn(a, b, precision=None):
    return lax.dot_general(
        a, b, (((0,), (0,)), ((), ())), precision=precision, preferred_element_type=F32
    )


def ids(shape, dim):
    return lax.broadcasted_iota(jnp.int32, shape, dim)


def far_first(side):
    return sorted(range(1, side), key=lambda k: -min(k, side - k))


def split_two(x):
    head = x.astype(BF16)
    return head, (x - head.astype(F32)).astype(BF16)


def entry_of(arrived, side, place, rate_re, rate_im, q):
    real = arrived[pl.ds(q, side, stride=16), :]
    imag = arrived[pl.ds(4 + q, side, stride=16), :]
    step = arrived[pl.ds(8 + q, side, stride=16), :]
    row = ids((side, LANES), 0)
    since = jnp.zeros((side, LANES), F32)
    for k in range(side):
        since = since + jnp.where((row < k) & (place > k), step[k : k + 1], 0.0)
    turn_re, turn_im = keep_of(rate_re, rate_im, since)
    before = row < place
    got_re = jnp.where(before, turn_re * real - turn_im * imag, 0.0)
    got_im = jnp.where(before, turn_re * imag + turn_im * real, 0.0)
    ahead = jnp.where(before, step, 0.0)
    return (
        jnp.sum(got_re, axis=0, keepdims=True),
        jnp.sum(got_im, axis=0, keepdims=True),
        jnp.sum(ahead, axis=0, keepdims=True),
    )


def kernel(
    dims,
    tokens_hbm,
    value_hbm,
    gate_hbm,
    drive_hbm,
    convp_hbm,
    statep_hbm,
    gain_hbm,
    taps_hbm,
    conv_gain_hbm,
    log_step_hbm,
    shift_hbm,
    rate_re_hbm,
    rate_im_hbm,
    in_hbm,
    out_map_hbm,
    skip_hbm,
    start_hbm,
    out_ref,
    gain_ref,
    taps_ref,
    conv_gain_ref,
    log_step_ref,
    shift_ref,
    rate_re_ref,
    rate_im_ref,
    in_ref,
    out_map_ref,
    skip_ref,
    start_ref,
    tok,
    nrm,
    gd,
    gv,
    pz,
    py,
    wd,
    wvg,
    wo_conv,
    wo_state,
    dtx,
    kr,
    ki,
    cr,
    ci,
    mm,
    in_blocks,
    out_blocks,
    drv,
    drvp,
    gf,
    cm,
    halo,
    halo_send,
    st_all,
    st_rows,
    mc_send,
    mc_recv,
    my_all,
    mz_all,
    mix_all,
    conv_all,
    state_all,
    acc,
    sems,
):
    side, cols = dims
    rows, depth = tokens_hbm.shape
    planes = side // cols
    sp, x = lax.axis_index("sp"), lax.axis_index("tp")
    c = lax.rem(sp, 2)
    chip = lax.div(sp, 2)
    y, z = lax.rem(chip, side), lax.div(chip, side)
    count = 2 * side * side
    steps = rows // CHUNKS
    wide = 4 * LANES
    free = iter(range(sems.shape[0]))

    def new_sems(n):
        return [sems.at[next(free)] for _ in range(n)]

    def at(zz, yy, cc):
        return (zz * side + yy) * 2 + cc

    def turn(a, k):
        return lax.rem(a + k, side)

    mate = at(z, y, 1 - c)
    b_me, a_me = c * z + (1 - c) * y, c * y + (1 - c) * z

    def b_peer(b):
        return c * at(b, y, 1) + (1 - c) * at(z, b, 0)

    def a_peer(a):
        return c * at(z, a, 1) + (1 - c) * at(a, y, 0)

    beyond = lax.rem(sp + 2 * c - 1 + count, count)
    following = lax.rem(sp + 1, count)

    def copy(src, dst, send_sem, recv_sem, to_sp, to_x):
        return pltpu.make_async_remote_copy(
            src_ref=src,
            dst_ref=dst,
            send_sem=send_sem,
            recv_sem=recv_sem,
            device_id=(to_sp, to_x),
            device_id_type=MESH,
        )

    outgoing = []

    def group(total):
        (sem,) = new_sems(1)
        outgoing.append((total, sem))
        return sem

    def send(src, dst, send_sem, recv_sem, to_sp, to_x):
        copy(src, dst, send_sem, recv_sem, to_sp, to_x).start()

    def arrive(dst, recv_sem):
        copy(dst, dst, recv_sem, recv_sem, mate, x).wait_recv()

    barrier = pltpu.get_barrier_semaphore()

    def greet(to_sp, to_x):
        pl.semaphore_signal(barrier, inc=1, device_id=(to_sp, to_x), device_id_type=MESH)

    for k in far_first(side):
        greet(at(z, turn(y, k), c), x)
        greet(at(turn(z, k), y, c), x)
    for k in far_first(cols):
        greet(sp, lax.rem(x + k, cols))
    greet(beyond, x)
    greet(mate, x)

    pairs = [
        (drive_hbm, gd.at[c, a_me, b_me]),
        (value_hbm, gv.at[c, a_me, b_me, :, pl.ds(0, LANES)]),
        (gate_hbm, gv.at[c, a_me, b_me, :, pl.ds(LANES, LANES)]),
        (convp_hbm, pz.at[z, :, pl.ds(0, LANES)]),
        (statep_hbm, pz.at[z, :, pl.ds(LANES, LANES)]),
        (in_hbm, in_ref),
        (out_map_hbm, out_map_ref),
        (rate_re_hbm, rate_re_ref),
        (rate_im_hbm, rate_im_ref),
        (start_hbm, start_ref),
        (skip_hbm, skip_ref),
        (log_step_hbm, log_step_ref),
        (shift_hbm, shift_ref),
        (gain_hbm, gain_ref),
        (taps_hbm, taps_ref),
        (conv_gain_hbm, conv_gain_ref),
        (tokens_hbm, tok),
    ]
    own_copies = [
        pltpu.make_async_copy(src, dst, sem) for (src, dst), sem in zip(pairs, new_sems(len(pairs)))
    ]
    for one in own_copies:
        one.start()
    for one in own_copies[:5]:
        one.wait()

    pl.semaphore_wait(barrier, 2 * side + cols - 1)
    d1_all, v1_all, p1_all, p2_all = new_sems(4)
    here = gd.at[c, a_me, b_me]
    sem = group(gd.at[c, a_me, pl.ds(0, side - 1)])
    for k in far_first(side):
        send(here, here, sem, d1_all, b_peer(turn(b_me, k)), x)
    here = gv.at[c, a_me, b_me]
    sem = group(gv.at[c, a_me, pl.ds(0, side - 1)])
    for k in far_first(side):
        send(here, here, sem, v1_all, b_peer(turn(b_me, k)), x)
    here = pz.at[z]
    sem = group(pz.at[pl.ds(0, side - 1)])
    for k in far_first(side):
        send(here, here, sem, p1_all, at(turn(z, k), y, c), x)

    for one in own_copies[5:13]:
        one.wait()
    group_mask = (ids((LANES, wide), 1) // 64 == ids((LANES, wide), 0) // 16).astype(F32)
    spread = (ids((64, wide), 1) % 64 == ids((64, wide), 0)).astype(F32)
    for part in range(2):
        rows_here, cols_here = pl.ds(part * LANES, LANES), pl.ds(part * wide, wide)
        first, rest = split_two(nn(in_ref[rows_here, :], spread, HIGHEST) * group_mask)
        in_blocks[part, pl.ds(0, LANES), :] = first
        in_blocks[part, pl.ds(LANES, LANES), :] = rest
        sign = 1.0 - 2.0 * part
        first, rest = split_two(nn(out_map_ref[rows_here, :], spread, HIGHEST) * (sign * group_mask))
        out_blocks[pl.ds(0, LANES), cols_here] = first
        out_blocks[pl.ds(LANES, LANES), cols_here] = rest
    own_group = (ids((8, wide), 1) // 64 == ids((8, wide), 0)).astype(F32)

    def flat(value):
        return jnp.sum(nn(value, spread, HIGHEST) * own_group, axis=0, keepdims=True)

    rate_re, rate_im = flat(rate_re_ref[...]), flat(rate_im_ref[...])
    first_re, first_im = flat(start_ref[0:8, :]), flat(start_ref[8:16, :])
    size = rate_re * rate_re + rate_im * rate_im
    inv_re, inv_im = rate_re / size, rate_im / size
    spread16 = (ids((16, LANES), 1) % 16 == ids((16, LANES), 0)).astype(F32)
    own16 = (ids((8, LANES), 1) // 16 == ids((8, LANES), 0)).astype(F32)
    skip_row = jnp.sum(nn(skip_ref[...], spread16, HIGHEST) * own16, axis=0, keepdims=True)
    eye8 = ids((8, 8), 0) == ids((8, 8), 1)
    log_step = jnp.sum(jnp.where(eye8, log_step_ref[...], 0.0), axis=1, keepdims=True)
    dt = jnp.exp(log_step + shift_ref[...])

    def tile(v, q):
        return v[:, q * LANES : (q + 1) * LANES]

    for q in range(4):
        dtx[q] = tn(dt, tile(own_group, q), HIGHEST)

    for one in own_copies[13:]:
        one.wait()
    gain = gain_ref[...]

    def norm_rows(i, carry):
        r = pl.ds(pl.multiple_of(i * 16, 16), 16)
        wide_rows = tok[r, :].astype(F32)
        mean = jnp.sum(wide_rows * wide_rows, axis=1, keepdims=True) * (1.0 / depth)
        nrm[r, :] = (wide_rows * lax.rsqrt(mean + 1e-06) * gain).astype(BF16)
        return carry

    lax.fori_loop(0, rows // 16, norm_rows, 0, unroll=4)

    d2_from, v2_from = new_sems(side - 1), new_sems(side - 1)
    dc_all, vc_all, pc_all = new_sems(3)
    arrive(gd.at[c, a_me, pl.ds(0, side - 1)], d1_all)
    line = gd.at[c, a_me]
    sem, dc_sem = group(gd.at[c, pl.ds(0, side - 1)]), group(gd.at[c])
    for k in far_first(side):
        send(line, line, sem, d2_from[k - 1], a_peer(turn(a_me, k)), x)
    send(line, line, dc_sem, dc_all, mate, x)

    arrive(gv.at[c, a_me, pl.ds(0, side - 1)], v1_all)
    line = gv.at[c, a_me]
    sem, vc_sem = group(gv.at[c, pl.ds(0, side - 1)]), group(gv.at[c])
    for k in far_first(side):
        send(line, line, sem, v2_from[k - 1], a_peer(turn(a_me, k)), x)
    send(line, line, vc_sem, vc_all, mate, x)
    arrive(pz.at[pl.ds(0, side - 1)], p1_all)
    sem = group(pz.at[pl.ds(0, (cols - 1) * planes)])
    for k in far_first(cols):
        to = lax.rem(x + k, cols)
        send(pz.at[pl.ds(to * planes, planes)], py.at[c, y, x], sem, p2_all, sp, to)
    py[c, y, x] = pz[pl.ds(x * planes, planes)]

    def keep_rows(j, carry):
        r = pl.ds(pl.multiple_of(j * 8, 8), 8)
        new = []
        for q in range(4):
            step = dtx[q, pl.ds(j, CHUNKS, stride=steps), :]
            keep_re, keep_im = keep_of(tile(rate_re, q), tile(rate_im, q), step)
            minus = keep_re - 1.0
            cols_q = pl.ds(q * LANES, LANES)
            kr[r, cols_q] = keep_re
            ki[r, cols_q] = keep_im
            cr[r, cols_q] = minus * tile(inv_re, q) + keep_im * tile(inv_im, q)
            ci[r, cols_q] = keep_im * tile(inv_re, q) - minus * tile(inv_im, q)
            new.append(carry[q] + step)
        return tuple(new)

    zero = jnp.zeros((CHUNKS, LANES), F32)
    spans = lax.fori_loop(0, steps, keep_rows, (zero,) * 4, unroll=2)

    for k in reversed(far_first(side)):
        block = gd.at[c, turn(a_me, side - k)]
        arrive(block, d2_from[k - 1])
        send(block, block, dc_sem, dc_all, mate, x)

    arrive(gd.at[1 - c], dc_all)

    def place_drive(a, carry):
        for b in range(side):
            r = pl.multiple_of(at(a, b, 0) * 16, 16)
            wd[pl.ds(r, 16), :] = gd[0, a, b]
            r = pl.multiple_of(at(b, a, 1) * 16, 16)
            wd[pl.ds(r, 16), :] = gd[1, a, b]
        return carry

    lax.fori_loop(0, side, place_drive, 0)
    block_rows = min(rows, 256)

    def blocks(body):
        for i in range(rows // block_rows):
            body(pl.ds(i * block_rows, block_rows))

    def drive_rows(r):
        drv[r, :] = nn(nrm[r, :], wd[...]).astype(BF16).astype(F32)

    blocks(drive_rows)

    def turn_rows(j, carry):
        r = pl.ds(pl.multiple_of(j * 8, 8), 8)
        drvp[r, :] = drv[pl.ds(j, CHUNKS, stride=steps), :]
        return carry

    lax.fori_loop(0, steps, turn_rows, 0, unroll=8)

    def map_rows(r):
        d = drvp[r, :].astype(BF16)
        d = jnp.concatenate([d, d], axis=1)
        mm[r, pl.ds(0, wide)] = nn(d, in_blocks[0])
        mm[r, pl.ds(wide, wide)] = nn(d, in_blocks[1])

    blocks(map_rows)

    def scan_rows(j, carry):
        r = pl.ds(pl.multiple_of(j * 8, 8), 8)
        new = []
        for q in range(4):
            cols_q = pl.ds(q * LANES, LANES)
            s_re, s_im = carry[2 * q], carry[2 * q + 1]
            c_re, c_im = cr[r, cols_q], ci[r, cols_q]
            m_re, m_im = mm[r, cols_q], mm[r, pl.ds(wide + q * LANES, LANES)]
            u_re = c_re * m_re - c_im * m_im
            u_im = c_re * m_im + c_im * m_re
            cr[r, cols_q] = u_re
            ci[r, cols_q] = u_im
            k_re, k_im = kr[r, cols_q], ki[r, cols_q]
            new.append((k_re * s_re + u_re) - k_im * s_im)
            new.append((k_re * s_im + u_im) + k_im * s_re)
        return tuple(new)

    finals = lax.fori_loop(0, steps, scan_rows, (zero,) * 8, unroll=2)

    row8 = ids((CHUNKS, LANES), 0)
    starts, mine, ahead_spans = [], [], []
    for q in range(4):
        re_q, im_q = tile(rate_re, q), tile(rate_im, q)
        hop_re, hop_im = keep_of(re_q, im_q, spans[q])
        f_re, f_im = finals[2 * q], finals[2 * q + 1]
        e_re = e_im = total = jnp.zeros((1, LANES), F32)
        l_re = l_im = ahead = zero
        for s in range(CHUNKS):
            l_re = jnp.where(row8 == s, e_re, l_re)
            l_im = jnp.where(row8 == s, e_im, l_im)
            ahead = jnp.where(row8 == s, total, ahead)
            h_re, h_im = hop_re[s : s + 1], hop_im[s : s + 1]
            e_re, e_im = (
                h_re * e_re - h_im * e_im + f_re[s : s + 1],
                h_re * e_im + h_im * e_re + f_im[s : s + 1],
            )
            total = total + spans[q][s : s + 1]
        starts.append((l_re, l_im))
        ahead_spans.append(ahead)
        mine.append((e_re, e_im, total))
        mc_send[q : q + 1, :] = e_re
        mc_send[4 + q : 5 + q, :] = e_im
        mc_send[8 + q : 9 + q, :] = total
    mc_send[12:16, :] = jnp.zeros((4, LANES), F32)
    mc_in, halo_in, cy_all, cz_all = new_sems(4)
    send(mc_send, mc_recv, group(mc_send), mc_in, mate, x)

    arrive(mc_recv, mc_in)
    core_entry = []
    second = c == 1
    slot = pl.multiple_of(y * 16, 16)
    for q in range(4):
        re_q, im_q = tile(rate_re, q), tile(rate_im, q)
        m_re, m_im, m_span = mine[q]
        o_re, o_im = mc_recv[q : q + 1, :], mc_recv[4 + q : 5 + q, :]
        o_span = mc_recv[8 + q : 9 + q, :]
        a_re, a_im = jnp.where(second, o_re, m_re), jnp.where(second, o_im, m_im)
        b_re, b_im = jnp.where(second, m_re, o_re), jnp.where(second, m_im, o_im)
        h_re, h_im = keep_of(re_q, im_q, jnp.where(second, m_span, o_span))
        my_all[pl.ds(slot + q, 1), :] = h_re * a_re - h_im * a_im + b_re
        my_all[pl.ds(slot + 4 + q, 1), :] = h_re * a_im + h_im * a_re + b_im
        my_all[pl.ds(slot + 8 + q, 1), :] = m_span + o_span
        none = jnp.zeros_like(o_re)
        core_entry.append(
            (
                jnp.where(second, o_re, none),
                jnp.where(second, o_im, none),
                jnp.where(second, o_span, none),
            )
        )
    part_rows = (side - 1) * 12
    here = my_all.at[pl.ds(slot, 12), :]
    sem = group(my_all.at[pl.ds(0, part_rows), :])
    for k in far_first(side):
        send(here, here, sem, cy_all, at(z, turn(y, k), c), x)

    arrive(pz.at[pl.ds(0, (cols - 1) * planes)], p2_all)
    p3_from = new_sems(side)
    p3_sem, pc_sem = group(py.at[c, pl.ds(0, side - 1)]), group(py.at[c])
    heading = 1 - 2 * c
    ahead_steps, back_steps = side // 2, (side - 1) // 2

    def along(k):
        return lax.rem(y + k * heading + side, side)

    def ring(step):
        if step > 1:
            for k, order, steps_there in (
                (-(step - 1), step - 1, ahead_steps),
                (step - 1, ahead_steps + step - 1, back_steps),
            ):
                if step - 1 <= steps_there:
                    block = py.at[c, along(k)]
                    arrive(block, p3_from[order])
                    send(block, block, pc_sem, pc_all, mate, x)
        for k, order, steps_there, to in (
            (-(step - 1), step, ahead_steps, 1),
            (step - 1, ahead_steps + step, back_steps, -1),
        ):
            if step <= steps_there:
                block = py.at[c, along(k)]
                send(block, block, p3_sem, p3_from[order], at(z, along(to), c), x)

    ring(1)
    line = py.at[c, y]
    send(line, line, pc_sem, pc_all, mate, x)

    for k in reversed(far_first(side)):
        block = gv.at[c, turn(a_me, side - k)]
        arrive(block, v2_from[k - 1])
        send(block, block, vc_sem, vc_all, mate, x)

    arrive(gv.at[1 - c], vc_all)

    def place_value(a, carry):
        for b in range(side):
            r = pl.multiple_of(at(a, b, 0) * 16, 16)
            wvg[pl.ds(r, 16), :] = gv[0, a, b]
            r = pl.multiple_of(at(b, a, 1) * 16, 16)
            wvg[pl.ds(r, 16), :] = gv[1, a, b]
        return carry

    lax.fori_loop(0, side, place_value, 0)

    def gate_rows(r):
        both = nn(nrm[r, :], wvg[...]).astype(BF16).astype(F32)
        gated = (both[:, :LANES] * jax.nn.sigmoid(both[:, LANES:])).astype(BF16)
        gf[pl.ds(r.start + 32, block_rows), :] = gated.astype(F32)

    blocks(gate_rows)
    halo_send[...] = gf[rows : rows + 32, :].astype(BF16)
    send(halo_send, halo, group(halo_send), halo_in, following, x)

    arrive(my_all.at[pl.ds(0, part_rows), :], cy_all)
    chip_entry = []
    slot_z = pl.multiple_of(z * 16, 16)
    for q in range(4):
        re_q, im_q = tile(rate_re, q), tile(rate_im, q)
        chip_entry.append(entry_of(my_all, side, y, re_q, im_q, q))
        all_re, all_im, all_span = entry_of(my_all, side, side, re_q, im_q, q)
        mz_all[pl.ds(slot_z + q, 1), :] = all_re
        mz_all[pl.ds(slot_z + 4 + q, 1), :] = all_im
        mz_all[pl.ds(slot_z + 8 + q, 1), :] = all_span
    here = mz_all.at[pl.ds(slot_z, 12), :]
    sem = group(mz_all.at[pl.ds(0, part_rows), :])
    for k in far_first(side):
        send(here, here, sem, cz_all, at(turn(z, k), y, c), x)

    ring(2)

    arrive(halo, halo_in)

    gf[0:32, :] = jnp.where(sp == 0, 0.0, halo[...].astype(F32))
    taps = taps_ref.shape[0]
    conv_rows = min(rows, 64)

    def conv_block(i, carry):
        base = pl.multiple_of(i * conv_rows, conv_rows)
        total = jnp.zeros((conv_rows, LANES), F32)
        for k in range(taps):
            total = total + taps_ref[k : k + 1, :] * gf[pl.ds(base + (33 - taps) + k, conv_rows), :]
        cm[pl.ds(base, conv_rows), :] = total
        return carry

    lax.fori_loop(0, rows // conv_rows, conv_block, 0)

    mix = cm[...]
    own_mean = nn(mix, jnp.full((LANES, LANES), 1.0 / LANES, F32), HIGHEST)
    lane_x = pl.multiple_of(x * LANES, LANES)
    mix_all[:, pl.ds(lane_x, LANES)] = (mix - own_mean).astype(BF16)
    ones = jnp.ones((8, LANES), F32)
    row_st = ids((8, rows), 0)
    sums = nt(ones, mix, HIGHEST)
    squares = nt(ones, mix * mix, HIGHEST)
    st_all[x] = jnp.where(row_st == 0, sums, jnp.where(row_st == 1, squares, 0.0))
    st_all[x, 2:3, 0:LANES] = conv_gain_ref[...]
    (st_in,) = new_sems(1)
    here = st_all.at[x]
    sem = group(st_all.at[pl.ds(0, cols - 1)])
    for k in far_first(cols):
        send(here, here, sem, st_in, sp, lax.rem(x + k, cols))
    half = rows // 2
    right, left = lax.rem(x + 1, cols), lax.rem(x + cols - 1, cols)
    across = lax.rem(x + 2, cols)

    class Spread:
        def __init__(self, buffer):
            self.buffer = buffer
            self.sem = group(buffer.at[:, pl.ds(0, (cols - 1) * LANES)])
            self.arrivals = new_sems(6 if cols > 2 else 2)

        def part(self, col, first):
            lanes = pl.ds(pl.multiple_of(col * LANES, LANES), LANES)
            return self.buffer.at[pl.ds(0 if first else half, half), lanes]

        def push(self, col, first, order, to):
            block = self.part(col, first)
            send(block, block, self.sem, self.arrivals[order], sp, to)

        def pull(self, col, first, order):
            arrive(self.part(col, first), self.arrivals[order])

        def begin(self):
            self.push(x, 1, 0, right)
            if cols > 2:
                self.push(x, 0, 2, left)
            self.push(x, 0, 1, right)
            if cols > 2:
                self.push(x, 1, 3, left)

        def pass_on(self):
            if cols > 2:
                self.pull(left, 1, 0)
                self.push(left, 1, 4, right)
                self.pull(right, 0, 2)
                self.push(right, 0, 5, left)

        def finish(self):
            if cols == 2:
                self.pull(left, 1, 0)
            self.pull(left, 0, 1)
            if cols > 2:
                self.pull(right, 1, 3)
                self.pull(across, 1, 4)
                self.pull(across, 0, 5)

    mix_spread = Spread(mix_all)
    mix_spread.begin()

    ring(3)

    arrive(mz_all.at[pl.ds(0, part_rows), :], cz_all)

    begin = []
    for q in range(4):
        re_q, im_q = tile(rate_re, q), tile(rate_im, q)
        s_re, s_im = tile(first_re, q), tile(first_im, q)
        for more_re, more_im, span in (
            entry_of(mz_all, side, z, re_q, im_q, q),
            chip_entry[q],
            core_entry[q],
        ):
            h_re, h_im = keep_of(re_q, im_q, span)
            s_re, s_im = h_re * s_re - h_im * s_im + more_re, h_re * s_im + h_im * s_re + more_im
        h_re, h_im = keep_of(re_q, im_q, ahead_spans[q])
        begin.append(h_re * s_re - h_im * s_im + starts[q][0])
        begin.append(h_re * s_im + h_im * s_re + starts[q][1])

    ring(4)

    def state_rows(j, carry):
        r = pl.ds(pl.multiple_of(j * 8, 8), 8)
        new = []
        for q in range(4):
            cols_q = pl.ds(q * LANES, LANES)
            s_re, s_im = carry[2 * q], carry[2 * q + 1]
            k_re, k_im = kr[r, cols_q], ki[r, cols_q]
            n_re = (k_re * s_re + cr[r, cols_q]) - k_im * s_im
            n_im = (k_re * s_im + ci[r, cols_q]) + k_im * s_re
            mm[r, cols_q] = n_re
            mm[r, pl.ds(wide + q * LANES, LANES)] = n_im
            new.extend((n_re, n_im))
        return tuple(new)

    lax.fori_loop(0, steps, state_rows, tuple(begin), unroll=2)

    def read_rows(r):
        first, rest = split_two(mm[r, :])
        total = nt(first, out_blocks[...])
        total = total[:, :LANES] + total[:, LANES:] + nt(rest, out_blocks[pl.ds(0, LANES), :])
        drvp[r, :] = jax.nn.gelu(total + skip_row * drvp[r, :])

    blocks(read_rows)

    def back_rows(j, carry):
        r = pl.ds(pl.multiple_of(j * 8, 8), 8)
        drv[pl.ds(j, CHUNKS, stride=steps), :] = drvp[r, :]
        return carry

    lax.fori_loop(0, steps, back_rows, 0, unroll=8)
    state_all[:, pl.ds(lane_x, LANES)] = drv[...].astype(BF16)

    mix_spread.pass_on()
    state_spread = Spread(state_all)
    state_spread.begin()

    for step in range(5, ahead_steps + 2):
        ring(step)

    arrive(st_all.at[pl.ds(0, cols - 1)], st_in)
    channels = cols * LANES
    mean = sum(st_all[k, 0:1, :] for k in range(cols)) * (1.0 / channels)
    square = sum(st_all[k, 1:2, :] for k in range(cols)) * (1.0 / channels)
    inv = lax.rsqrt(square - mean * mean + 1e-05)
    table = jnp.where(row_st == 0, inv, 0.0)
    for k in range(cols):
        offset = (st_all[k, 0:1, :] * (1.0 / LANES) - mean) * inv
        table = jnp.where(row_st == 1 + k, offset, table)
    st_rows[...] = table
    pick = ids((8, LANES), 0)

    def apply_norm(col):
        lanes = pl.ds(pl.multiple_of(col * LANES, LANES), LANES)
        scale = tn(st_rows[...], (pick == 0).astype(F32), HIGHEST)
        offset = tn(st_rows[...], (pick == 1 + col).astype(F32), HIGHEST)
        value = mix_all[:, lanes].astype(F32) * scale + offset
        value = value * st_all[col, 2:3, 0:LANES]
        conv_all[:, lanes] = (value * jax.nn.sigmoid(value)).astype(BF16)

    apply_norm(x)

    state_spread.pass_on()

    mix_spread.finish()

    for k in range(1, cols):
        apply_norm(lax.rem(x + k, cols))

    arrive(py.at[1 - c], pc_all)

    def place_out(b, carry):
        for core in range(2):
            for col in range(cols):
                for plane in range(planes):
                    r = pl.ds(pl.multiple_of((plane * side + b) * 32 + core * 16, 16), 16)
                    piece = py[core, b, col, plane]
                    wo_conv[r, pl.ds(col * LANES, LANES)] = piece[:, :LANES]
                    wo_state[r, pl.ds(col * LANES, LANES)] = piece[:, LANES:]
        return carry

    lax.fori_loop(0, side, place_out, 0)

    def early_rows(r):
        acc[r, :] = nt(conv_all[r, :], wo_conv[...])

    blocks(early_rows)

    state_spread.finish()

    def late_rows(r):
        out_ref[r, :] = (acc[r, :] + nt(state_all[r, :], wo_state[...])).astype(BF16)

    blocks(late_rows)

    for total, sem in outgoing:
        copy(total, total, sem, sem, mate, x).wait_send()
    assert next(free, None) is None


def sem_count(side, cols):
    operands, groups = 17, 17
    return operands + groups + 2 * (side - 1) + side + 3 + 4 + 4 + 1 + 2 * (6 if cols > 2 else 2)


def on_device(
    side,
    cols,
    tokens,
    norm_gain,
    w_value,
    w_gate,
    w_drive,
    conv_taps,
    conv_gain,
    log_step,
    step_shift,
    state_real,
    state_imag,
    in_map,
    out_map,
    skip_gain,
    start_state,
    conv_proj,
    state_proj,
):
    rows, depth = tokens.shape
    planes = side // cols
    out_cols = planes * side * 32
    groups, states = state_real.shape
    width = groups * states
    hbm = pl.BlockSpec(memory_space=pl.ANY)
    vmem = pl.BlockSpec(memory_space=pltpu.VMEM)
    small = (
        norm_gain.reshape(1, depth),
        conv_taps,
        conv_gain.reshape(1, -1),
        log_step.reshape(1, -1),
        step_shift.T,
        state_real,
        state_imag,
        jnp.transpose(in_map, (0, 1, 3, 2)).reshape(-1, states),
        out_map.reshape(-1, states),
        skip_gain,
        start_state.reshape(-1, states),
    )
    return pl.pallas_call(
        functools.partial(kernel, (side, cols)),
        out_shape=pltpu.VMEM((rows, out_cols), BF16),
        in_specs=[hbm] * 17,
        out_specs=vmem,
        scratch_shapes=[
            *[pltpu.VMEM(a.shape, F32) for a in small],
            pltpu.VMEM((rows, depth), BF16),
            pltpu.VMEM((rows, depth), BF16),
            pltpu.VMEM((2, side, side, 16, LANES), BF16),
            pltpu.VMEM((2, side, side, 16, 2 * LANES), BF16),
            pltpu.VMEM((side, 16, 2 * LANES), BF16),
            pltpu.VMEM((2, side, cols, planes, 16, 2 * LANES), BF16),
            pltpu.VMEM((depth, LANES), BF16),
            pltpu.VMEM((depth, 2 * LANES), BF16),
            pltpu.VMEM((out_cols, cols * LANES), BF16),
            pltpu.VMEM((out_cols, cols * LANES), BF16),
            pltpu.VMEM((4, rows, LANES), F32),
            *[pltpu.VMEM((rows, width), F32)] * 4,
            pltpu.VMEM((rows, 2 * width), F32),
            pltpu.VMEM((2, 2 * LANES, width), BF16),
            pltpu.VMEM((2 * LANES, 2 * width), BF16),
            pltpu.VMEM((rows, LANES), F32),
            pltpu.VMEM((rows, LANES), F32),
            pltpu.VMEM((rows + 32, LANES), F32),
            pltpu.VMEM((rows, LANES), F32),
            pltpu.VMEM((32, LANES), BF16),
            pltpu.VMEM((32, LANES), BF16),
            pltpu.VMEM((cols, 8, rows), F32),
            pltpu.VMEM((8, rows), F32),
            pltpu.VMEM((16, LANES), F32),
            pltpu.VMEM((16, LANES), F32),
            pltpu.VMEM((side * 16, LANES), F32),
            pltpu.VMEM((side * 16, LANES), F32),
            *[pltpu.VMEM((rows, cols * LANES), BF16)] * 3,
            pltpu.VMEM((rows, out_cols), F32),
            pltpu.SemaphoreType.DMA((sem_count(side, cols),)),
        ],
        compiler_params=pltpu.CompilerParams(
            collective_id=0, has_side_effects=True, vmem_limit_bytes=60 * 1024 * 1024
        ),
    )(
        tokens,
        w_value,
        w_gate,
        w_drive,
        conv_proj.T,
        state_proj.T,
        *small,
    )


def solution(mesh):
    side = math.isqrt(mesh.shape["sp"] // 2)
    placed = (
        P("sp", None),
        P(),
        P("sp", "tp"),
        P("sp", "tp"),
        P("sp", "tp"),
        P(None, "tp"),
        P("tp"),
        P("tp"),
        P("sp", "tp"),
        P("tp", None),
        P("tp", None),
        P(None, "tp", None, None),
        P(None, "tp", None, None),
        P("tp", None),
        P(None, "tp", None),
        P("tp", "sp"),
        P("tp", "sp"),
    )
    return jax.shard_map(
        functools.partial(on_device, side, mesh.shape["tp"]),
        mesh=mesh,
        in_specs=placed,
        out_specs=P("sp", "tp"),
        check_vma=False,
    )
```

```python
import functools
import math

import jax
import jax.numpy as jnp
from jax import lax
from jax.experimental import pallas as pl
from jax.experimental.pallas import tpu as pltpu
from jax.sharding import PartitionSpec as P

MESH = pl.DeviceIdType.MESH
F32, BF16 = jnp.float32, jnp.bfloat16
HIGHEST = lax.Precision.HIGHEST
CHUNKS = 8
LANES = 128
PI_HEAD, PI_MID, PI_TAIL = 3.140625, 9.67502593994140625e-4, 1.509957990978376432e-7
SIN = (
    0.9999999956945582,
    -0.16666657935421791,
    0.008333049779224343,
    -0.00019808982983932522,
    2.605019582042587e-06,
)
COS = (
    0.9999999997785899,
    -0.4999999935376166,
    0.04166663608814349,
    -0.0013888359276841241,
    2.476005397141232e-05,
    -2.6049608226484117e-07,
)


def series(terms, x):
    total = terms[-1]
    for term in reversed(terms[:-1]):
        total = total * x + term
    return total


def keep_of(rate_re, rate_im, step):
    angle = rate_im * step
    turns = jnp.floor(angle * (1.0 / math.pi) + 0.5)
    rest = ((angle - turns * PI_HEAD) - turns * PI_MID) - turns * PI_TAIL
    square = rest * rest
    half = turns * 0.5
    size = jnp.exp(rate_re * step) * (1.0 - 4.0 * (half - jnp.floor(half)))
    return size * series(COS, square), size * (rest * series(SIN, square))


def nn(a, b, precision=None):
    return lax.dot_general(
        a, b, (((1,), (0,)), ((), ())), precision=precision, preferred_element_type=F32
    )


def nt(a, b, precision=None):
    return lax.dot_general(
        a, b, (((1,), (1,)), ((), ())), precision=precision, preferred_element_type=F32
    )


def tn(a, b, precision=None):
    return lax.dot_general(
        a, b, (((0,), (0,)), ((), ())), precision=precision, preferred_element_type=F32
    )


def ids(shape, dim):
    return lax.broadcasted_iota(jnp.int32, shape, dim)


def far_first(side):
    return sorted(range(1, side), key=lambda k: -min(k, side - k))


def split_two(x):
    head = x.astype(BF16)
    return head, (x - head.astype(F32)).astype(BF16)


def entry_of(arrived, side, place, rate_re, rate_im, q):
    real = arrived[pl.ds(q, side, stride=16), :]
    imag = arrived[pl.ds(4 + q, side, stride=16), :]
    step = arrived[pl.ds(8 + q, side, stride=16), :]
    row = ids((side, LANES), 0)
    since = jnp.zeros((side, LANES), F32)
    for k in range(side):
        since = since + jnp.where((row < k) & (place > k), step[k : k + 1], 0.0)
    turn_re, turn_im = keep_of(rate_re, rate_im, since)
    before = row < place
    got_re = jnp.where(before, turn_re * real - turn_im * imag, 0.0)
    got_im = jnp.where(before, turn_re * imag + turn_im * real, 0.0)
    ahead = jnp.where(before, step, 0.0)
    return (
        jnp.sum(got_re, axis=0, keepdims=True),
        jnp.sum(got_im, axis=0, keepdims=True),
        jnp.sum(ahead, axis=0, keepdims=True),
    )


def kernel(
    dims,
    tokens_hbm,
    value_hbm,
    gate_hbm,
    drive_hbm,
    convp_hbm,
    statep_hbm,
    gain_hbm,
    taps_hbm,
    conv_gain_hbm,
    log_step_hbm,
    shift_hbm,
    rate_re_hbm,
    rate_im_hbm,
    in_hbm,
    out_map_hbm,
    skip_hbm,
    start_hbm,
    out_ref,
    gain_ref,
    taps_ref,
    conv_gain_ref,
    log_step_ref,
    shift_ref,
    rate_re_ref,
    rate_im_ref,
    in_ref,
    out_map_ref,
    skip_ref,
    start_ref,
    tok,
    nrm,
    gd,
    gv,
    pz,
    gp,
    wd,
    wvg,
    wo_conv,
    wo_state,
    dtx,
    kr,
    ki,
    cr,
    ci,
    mm,
    in_blocks,
    out_blocks,
    drv,
    drvp,
    gf,
    cm,
    halo,
    halo_send,
    st_all,
    st_rows,
    mc_send,
    mc_recv,
    my_all,
    mz_all,
    mix_all,
    conv_all,
    state_all,
    acc,
    sems,
):
    side, cols = dims
    rows, depth = tokens_hbm.shape
    planes = side // cols
    sp, x = lax.axis_index("sp"), lax.axis_index("tp")
    c = lax.rem(sp, 2)
    chip = lax.div(sp, 2)
    y, z = lax.rem(chip, side), lax.div(chip, side)
    count = 2 * side * side
    steps = rows // CHUNKS
    wide = 4 * LANES
    free = iter(range(sems.shape[0]))

    def new_sems(n):
        return [sems.at[next(free)] for _ in range(n)]

    def at(zz, yy, cc):
        return (zz * side + yy) * 2 + cc

    def turn(a, k):
        return lax.rem(a + k, side)

    mate = at(z, y, 1 - c)
    b_me, a_me = c * z + (1 - c) * y, c * y + (1 - c) * z

    def b_peer(b):
        return c * at(b, y, 1) + (1 - c) * at(z, b, 0)

    def a_peer(a):
        return c * at(z, a, 1) + (1 - c) * at(a, y, 0)

    shift = side // 2
    piece_z = lax.rem(lax.rem(z, planes) * cols + x + shift, side)
    piece_x = lax.div(z, planes)
    piece_a, piece_b = c * y + (1 - c) * piece_z, c * piece_z + (1 - c) * y
    order = lax.rem(z + side - shift, side)
    from_z, from_x = x * planes + lax.div(order, cols), lax.rem(order, cols)

    beyond = lax.rem(sp + 2 * c - 1 + count, count)
    following = lax.rem(sp + 1, count)

    def copy(src, dst, send_sem, recv_sem, to_sp, to_x):
        return pltpu.make_async_remote_copy(
            src_ref=src,
            dst_ref=dst,
            send_sem=send_sem,
            recv_sem=recv_sem,
            device_id=(to_sp, to_x),
            device_id_type=MESH,
        )

    outgoing = []

    def group(total):
        (sem,) = new_sems(1)
        outgoing.append((total, sem))
        return sem

    def send(src, dst, send_sem, recv_sem, to_sp, to_x):
        copy(src, dst, send_sem, recv_sem, to_sp, to_x).start()

    def arrive(dst, recv_sem):
        copy(dst, dst, recv_sem, recv_sem, mate, x).wait_recv()

    barrier = pltpu.get_barrier_semaphore()

    def greet(to_sp, to_x):
        pl.semaphore_signal(barrier, inc=1, device_id=(to_sp, to_x), device_id_type=MESH)

    for k in far_first(side):
        greet(at(z, turn(y, k), c), x)
        greet(at(turn(z, k), y, c), x)
    for k in far_first(cols):
        greet(sp, lax.rem(x + k, cols))
    greet(at(piece_z, y, c), piece_x)
    greet(at(from_z, y, c), from_x)
    greet(beyond, x)
    greet(mate, x)

    pairs = [
        (drive_hbm, gd.at[c, a_me, b_me]),
        (value_hbm, gv.at[c, a_me, b_me, :, pl.ds(0, LANES)]),
        (gate_hbm, gv.at[c, a_me, b_me, :, pl.ds(LANES, LANES)]),
        (convp_hbm, pz.at[:, pl.ds(0, LANES)]),
        (statep_hbm, pz.at[:, pl.ds(LANES, LANES)]),
        (in_hbm, in_ref),
        (out_map_hbm, out_map_ref),
        (rate_re_hbm, rate_re_ref),
        (rate_im_hbm, rate_im_ref),
        (start_hbm, start_ref),
        (skip_hbm, skip_ref),
        (log_step_hbm, log_step_ref),
        (shift_hbm, shift_ref),
        (gain_hbm, gain_ref),
        (taps_hbm, taps_ref),
        (conv_gain_hbm, conv_gain_ref),
        (tokens_hbm, tok),
    ]
    own_copies = [
        pltpu.make_async_copy(src, dst, sem) for (src, dst), sem in zip(pairs, new_sems(len(pairs)))
    ]
    for one in own_copies:
        one.start()
    for one in own_copies[:5]:
        one.wait()

    pl.semaphore_wait(barrier, 2 * side + cols + 1)
    d1_all, v1_all, p0_in, p1_all = new_sems(4)
    here = gd.at[c, a_me, b_me]
    sem = group(gd.at[c, a_me, pl.ds(0, side - 1)])
    for k in far_first(side):
        send(here, here, sem, d1_all, b_peer(turn(b_me, k)), x)
    here = gv.at[c, a_me, b_me]
    sem = group(gv.at[c, a_me, pl.ds(0, side - 1)])
    for k in far_first(side):
        send(here, here, sem, v1_all, b_peer(turn(b_me, k)), x)
    send(pz, gp.at[c, piece_a, piece_b], group(pz), p0_in, at(piece_z, y, c), piece_x)

    for one in own_copies[5:13]:
        one.wait()
    group_mask = (ids((LANES, wide), 1) // 64 == ids((LANES, wide), 0) // 16).astype(F32)
    spread = (ids((64, wide), 1) % 64 == ids((64, wide), 0)).astype(F32)
    for part in range(2):
        rows_here, cols_here = pl.ds(part * LANES, LANES), pl.ds(part * wide, wide)
        first, rest = split_two(nn(in_ref[rows_here, :], spread, HIGHEST) * group_mask)
        in_blocks[part, pl.ds(0, LANES), :] = first
        in_blocks[part, pl.ds(LANES, LANES), :] = rest
        sign = 1.0 - 2.0 * part
        first, rest = split_two(nn(out_map_ref[rows_here, :], spread, HIGHEST) * (sign * group_mask))
        out_blocks[pl.ds(0, LANES), cols_here] = first
        out_blocks[pl.ds(LANES, LANES), cols_here] = rest
    own_group = (ids((8, wide), 1) // 64 == ids((8, wide), 0)).astype(F32)

    def flat(value):
        return jnp.sum(nn(value, spread, HIGHEST) * own_group, axis=0, keepdims=True)

    rate_re, rate_im = flat(rate_re_ref[...]), flat(rate_im_ref[...])
    first_re, first_im = flat(start_ref[0:8, :]), flat(start_ref[8:16, :])
    size = rate_re * rate_re + rate_im * rate_im
    inv_re, inv_im = rate_re / size, rate_im / size
    spread16 = (ids((16, LANES), 1) % 16 == ids((16, LANES), 0)).astype(F32)
    own16 = (ids((8, LANES), 1) // 16 == ids((8, LANES), 0)).astype(F32)
    skip_row = jnp.sum(nn(skip_ref[...], spread16, HIGHEST) * own16, axis=0, keepdims=True)
    eye8 = ids((8, 8), 0) == ids((8, 8), 1)
    log_step = jnp.sum(jnp.where(eye8, log_step_ref[...], 0.0), axis=1, keepdims=True)
    dt = jnp.exp(log_step + shift_ref[...])

    def tile(v, q):
        return v[:, q * LANES : (q + 1) * LANES]

    for q in range(4):
        dtx[q] = tn(dt, tile(own_group, q), HIGHEST)

    for one in own_copies[13:]:
        one.wait()
    gain = gain_ref[...]

    def norm_rows(i, carry):
        r = pl.ds(pl.multiple_of(i * 16, 16), 16)
        wide_rows = tok[r, :].astype(F32)
        mean = jnp.sum(wide_rows * wide_rows, axis=1, keepdims=True) * (1.0 / depth)
        nrm[r, :] = (wide_rows * lax.rsqrt(mean + 1e-06) * gain).astype(BF16)
        return carry

    lax.fori_loop(0, rows // 16, norm_rows, 0, unroll=4)

    d2_from, v2_from, p2_from = (new_sems(side - 1) for _ in range(3))
    dc_all, vc_all, pc_all = new_sems(3)
    arrive(gd.at[c, a_me, pl.ds(0, side - 1)], d1_all)
    line = gd.at[c, a_me]
    sem, dc_sem = group(gd.at[c, pl.ds(0, side - 1)]), group(gd.at[c])
    for k in far_first(side):
        send(line, line, sem, d2_from[k - 1], a_peer(turn(a_me, k)), x)
    send(line, line, dc_sem, dc_all, mate, x)

    arrive(gv.at[c, a_me, pl.ds(0, side - 1)], v1_all)
    line = gv.at[c, a_me]
    sem, vc_sem = group(gv.at[c, pl.ds(0, side - 1)]), group(gv.at[c])
    for k in far_first(side):
        send(line, line, sem, v2_from[k - 1], a_peer(turn(a_me, k)), x)
    send(line, line, vc_sem, vc_all, mate, x)
    here = gp.at[c, a_me, b_me]
    arrive(here, p0_in)
    sem = group(gp.at[c, a_me, pl.ds(0, side - 1)])
    for k in far_first(side):
        send(here, here, sem, p1_all, b_peer(turn(b_me, k)), x)

    def keep_rows(j, carry):
        r = pl.ds(pl.multiple_of(j * 8, 8), 8)
        new = []
        for q in range(4):
            step = dtx[q, pl.ds(j, CHUNKS, stride=steps), :]
            keep_re, keep_im = keep_of(tile(rate_re, q), tile(rate_im, q), step)
            minus = keep_re - 1.0
            cols_q = pl.ds(q * LANES, LANES)
            kr[r, cols_q] = keep_re
            ki[r, cols_q] = keep_im
            cr[r, cols_q] = minus * tile(inv_re, q) + keep_im * tile(inv_im, q)
            ci[r, cols_q] = keep_im * tile(inv_re, q) - minus * tile(inv_im, q)
            new.append(carry[q] + step)
        return tuple(new)

    zero = jnp.zeros((CHUNKS, LANES), F32)
    spans = lax.fori_loop(0, steps, keep_rows, (zero,) * 4, unroll=2)

    for k in reversed(far_first(side)):
        block = gd.at[c, turn(a_me, side - k)]
        arrive(block, d2_from[k - 1])
        send(block, block, dc_sem, dc_all, mate, x)

    arrive(gd.at[1 - c], dc_all)

    def place_drive(a, carry):
        for b in range(side):
            r = pl.multiple_of(at(a, b, 0) * 16, 16)
            wd[pl.ds(r, 16), :] = gd[0, a, b]
            r = pl.multiple_of(at(b, a, 1) * 16, 16)
            wd[pl.ds(r, 16), :] = gd[1, a, b]
        return carry

    lax.fori_loop(0, side, place_drive, 0)
    block_rows = min(rows, 256)

    def blocks(body):
        for i in range(rows // block_rows):
            body(pl.ds(i * block_rows, block_rows))

    def drive_rows(r):
        drv[r, :] = nn(nrm[r, :], wd[...]).astype(BF16).astype(F32)

    blocks(drive_rows)

    def turn_rows(j, carry):
        r = pl.ds(pl.multiple_of(j * 8, 8), 8)
        drvp[r, :] = drv[pl.ds(j, CHUNKS, stride=steps), :]
        return carry

    lax.fori_loop(0, steps, turn_rows, 0, unroll=8)

    def map_rows(r):
        d = drvp[r, :].astype(BF16)
        d = jnp.concatenate([d, d], axis=1)
        mm[r, pl.ds(0, wide)] = nn(d, in_blocks[0])
        mm[r, pl.ds(wide, wide)] = nn(d, in_blocks[1])

    blocks(map_rows)

    def scan_rows(j, carry):
        r = pl.ds(pl.multiple_of(j * 8, 8), 8)
        new = []
        for q in range(4):
            cols_q = pl.ds(q * LANES, LANES)
            s_re, s_im = carry[2 * q], carry[2 * q + 1]
            c_re, c_im = cr[r, cols_q], ci[r, cols_q]
            m_re, m_im = mm[r, cols_q], mm[r, pl.ds(wide + q * LANES, LANES)]
            u_re = c_re * m_re - c_im * m_im
            u_im = c_re * m_im + c_im * m_re
            cr[r, cols_q] = u_re
            ci[r, cols_q] = u_im
            k_re, k_im = kr[r, cols_q], ki[r, cols_q]
            new.append((k_re * s_re + u_re) - k_im * s_im)
            new.append((k_re * s_im + u_im) + k_im * s_re)
        return tuple(new)

    finals = lax.fori_loop(0, steps, scan_rows, (zero,) * 8, unroll=2)

    row8 = ids((CHUNKS, LANES), 0)
    starts, mine, ahead_spans = [], [], []
    for q in range(4):
        re_q, im_q = tile(rate_re, q), tile(rate_im, q)
        hop_re, hop_im = keep_of(re_q, im_q, spans[q])
        f_re, f_im = finals[2 * q], finals[2 * q + 1]
        e_re = e_im = total = jnp.zeros((1, LANES), F32)
        l_re = l_im = ahead = zero
        for s in range(CHUNKS):
            l_re = jnp.where(row8 == s, e_re, l_re)
            l_im = jnp.where(row8 == s, e_im, l_im)
            ahead = jnp.where(row8 == s, total, ahead)
            h_re, h_im = hop_re[s : s + 1], hop_im[s : s + 1]
            e_re, e_im = (
                h_re * e_re - h_im * e_im + f_re[s : s + 1],
                h_re * e_im + h_im * e_re + f_im[s : s + 1],
            )
            total = total + spans[q][s : s + 1]
        starts.append((l_re, l_im))
        ahead_spans.append(ahead)
        mine.append((e_re, e_im, total))
        mc_send[q : q + 1, :] = e_re
        mc_send[4 + q : 5 + q, :] = e_im
        mc_send[8 + q : 9 + q, :] = total
    mc_send[12:16, :] = jnp.zeros((4, LANES), F32)
    mc_in, halo_in, cy_all = new_sems(3)
    cz_from, cz_sems = new_sems(side - 1), new_sems(side - 1)
    send(mc_send, mc_recv, group(mc_send), mc_in, mate, x)

    def hand_over_value(ks):
        for k in ks:
            block = gv.at[c, turn(a_me, side - k)]
            arrive(block, v2_from[k - 1])
            send(block, block, vc_sem, vc_all, mate, x)

    near_first = far_first(side)[::-1]
    hand_over_value(near_first[: side // 2])

    arrive(mc_recv, mc_in)
    core_entry = []
    second = c == 1
    slot = pl.multiple_of(y * 16, 16)
    for q in range(4):
        re_q, im_q = tile(rate_re, q), tile(rate_im, q)
        m_re, m_im, m_span = mine[q]
        o_re, o_im = mc_recv[q : q + 1, :], mc_recv[4 + q : 5 + q, :]
        o_span = mc_recv[8 + q : 9 + q, :]
        a_re, a_im = jnp.where(second, o_re, m_re), jnp.where(second, o_im, m_im)
        b_re, b_im = jnp.where(second, m_re, o_re), jnp.where(second, m_im, o_im)
        h_re, h_im = keep_of(re_q, im_q, jnp.where(second, m_span, o_span))
        my_all[pl.ds(slot + q, 1), :] = h_re * a_re - h_im * a_im + b_re
        my_all[pl.ds(slot + 4 + q, 1), :] = h_re * a_im + h_im * a_re + b_im
        my_all[pl.ds(slot + 8 + q, 1), :] = m_span + o_span
        none = jnp.zeros_like(o_re)
        core_entry.append(
            (
                jnp.where(second, o_re, none),
                jnp.where(second, o_im, none),
                jnp.where(second, o_span, none),
            )
        )
    part_rows = (side - 1) * 12
    here = my_all.at[pl.ds(slot, 12), :]
    sem = group(my_all.at[pl.ds(0, part_rows), :])
    for k in far_first(side):
        send(here, here, sem, cy_all, at(z, turn(y, k), c), x)

    hand_over_value(near_first[side // 2 :])

    arrive(gv.at[1 - c], vc_all)

    def place_value(a, carry):
        for b in range(side):
            r = pl.multiple_of(at(a, b, 0) * 16, 16)
            wvg[pl.ds(r, 16), :] = gv[0, a, b]
            r = pl.multiple_of(at(b, a, 1) * 16, 16)
            wvg[pl.ds(r, 16), :] = gv[1, a, b]
        return carry

    lax.fori_loop(0, side, place_value, 0)

    def gate_rows(r):
        both = nn(nrm[r, :], wvg[...]).astype(BF16).astype(F32)
        gated = (both[:, :LANES] * jax.nn.sigmoid(both[:, LANES:])).astype(BF16)
        gf[pl.ds(r.start + 32, block_rows), :] = gated.astype(F32)

    blocks(gate_rows)
    halo_send[...] = gf[rows : rows + 32, :].astype(BF16)
    send(halo_send, halo, group(halo_send), halo_in, following, x)

    arrive(my_all.at[pl.ds(0, part_rows), :], cy_all)
    chip_entry = []
    slot_z = pl.multiple_of(z * 16, 16)
    for q in range(4):
        re_q, im_q = tile(rate_re, q), tile(rate_im, q)
        chip_entry.append(entry_of(my_all, side, y, re_q, im_q, q))
        all_re, all_im, all_span = entry_of(my_all, side, side, re_q, im_q, q)
        mz_all[pl.ds(slot_z + q, 1), :] = all_re
        mz_all[pl.ds(slot_z + 4 + q, 1), :] = all_im
        mz_all[pl.ds(slot_z + 8 + q, 1), :] = all_span
    here = mz_all.at[pl.ds(slot_z, 12), :]
    for k in range(side - 1, 0, -1):

        @pl.when(z + k < side)
        def _():
            send(here, here, cz_sems[k - 1], cz_from[k - 1], at(lax.rem(z + k, side), y, c), x)

    arrive(gp.at[c, a_me, pl.ds(0, side - 1)], p1_all)
    line = gp.at[c, a_me]
    sem, pc_sem = group(gp.at[c, pl.ds(0, side - 1)]), group(gp.at[c])
    for k in far_first(side):
        send(line, line, sem, p2_from[k - 1], a_peer(turn(a_me, k)), x)
    send(line, line, pc_sem, pc_all, mate, x)

    arrive(halo, halo_in)

    gf[0:32, :] = jnp.where(sp == 0, 0.0, halo[...].astype(F32))
    taps = taps_ref.shape[0]
    conv_rows = min(rows, 64)

    def conv_block(i, carry):
        base = pl.multiple_of(i * conv_rows, conv_rows)
        total = jnp.zeros((conv_rows, LANES), F32)
        for k in range(taps):
            total = total + taps_ref[k : k + 1, :] * gf[pl.ds(base + (33 - taps) + k, conv_rows), :]
        cm[pl.ds(base, conv_rows), :] = total
        return carry

    lax.fori_loop(0, rows // conv_rows, conv_block, 0)

    mix = cm[...]
    own_mean = nn(mix, jnp.full((LANES, LANES), 1.0 / LANES, F32), HIGHEST)
    lane_x = pl.multiple_of(x * LANES, LANES)
    mix_all[:, pl.ds(lane_x, LANES)] = (mix - own_mean).astype(BF16)
    half = rows // 2
    right, left = lax.rem(x + 1, cols), lax.rem(x + cols - 1, cols)
    across = lax.rem(x + 2, cols)

    class Spread:
        def __init__(self, buffer):
            self.buffer = buffer
            self.sem = group(buffer.at[:, pl.ds(0, (cols - 1) * LANES)])
            self.arrivals = new_sems(6 if cols > 2 else 2)

        def part(self, col, first):
            lanes = pl.ds(pl.multiple_of(col * LANES, LANES), LANES)
            return self.buffer.at[pl.ds(0 if first else half, half), lanes]

        def push(self, col, first, order, to):
            block = self.part(col, first)
            send(block, block, self.sem, self.arrivals[order], sp, to)

        def pull(self, col, first, order):
            arrive(self.part(col, first), self.arrivals[order])

        def begin(self):
            self.push(x, 1, 0, right)
            if cols > 2:
                self.push(x, 0, 2, left)
            self.push(x, 0, 1, right)
            if cols > 2:
                self.push(x, 1, 3, left)

        def pass_on(self):
            if cols > 2:
                self.pull(left, 1, 0)
                self.push(left, 1, 4, right)
                self.pull(right, 0, 2)
                self.push(right, 0, 5, left)

        def finish(self):
            if cols == 2:
                self.pull(left, 1, 0)
            self.pull(left, 0, 1)
            if cols > 2:
                self.pull(right, 1, 3)
                self.pull(across, 1, 4)
                self.pull(across, 0, 5)

    mix_spread = Spread(mix_all)
    mix_spread.begin()

    ones = jnp.ones((8, LANES), F32)
    row_st = ids((8, rows), 0)
    sums = nt(ones, mix, HIGHEST)
    squares = nt(ones, mix * mix, HIGHEST)
    st_all[x] = jnp.where(row_st == 0, sums, jnp.where(row_st == 1, squares, 0.0))
    st_all[x, 2:3, 0:LANES] = conv_gain_ref[...]
    (st_in,) = new_sems(1)
    here = st_all.at[x]
    sem = group(st_all.at[pl.ds(0, cols - 1)])
    for k in far_first(cols):
        send(here, here, sem, st_in, sp, lax.rem(x + k, cols))

    for k in range(1, side):

        @pl.when(z >= k)
        def _():
            from_slot = pl.multiple_of(lax.rem(z + side - k, side) * 16, 16)
            arrive(mz_all.at[pl.ds(from_slot, 12), :], cz_from[k - 1])


    begin = []
    for q in range(4):
        re_q, im_q = tile(rate_re, q), tile(rate_im, q)
        s_re, s_im = tile(first_re, q), tile(first_im, q)
        for more_re, more_im, span in (
            entry_of(mz_all, side, z, re_q, im_q, q),
            chip_entry[q],
            core_entry[q],
        ):
            h_re, h_im = keep_of(re_q, im_q, span)
            s_re, s_im = h_re * s_re - h_im * s_im + more_re, h_re * s_im + h_im * s_re + more_im
        h_re, h_im = keep_of(re_q, im_q, ahead_spans[q])
        begin.append(h_re * s_re - h_im * s_im + starts[q][0])
        begin.append(h_re * s_im + h_im * s_re + starts[q][1])

    def state_rows(j, carry):
        r = pl.ds(pl.multiple_of(j * 8, 8), 8)
        new = []
        for q in range(4):
            cols_q = pl.ds(q * LANES, LANES)
            s_re, s_im = carry[2 * q], carry[2 * q + 1]
            k_re, k_im = kr[r, cols_q], ki[r, cols_q]
            n_re = (k_re * s_re + cr[r, cols_q]) - k_im * s_im
            n_im = (k_re * s_im + ci[r, cols_q]) + k_im * s_re
            mm[r, cols_q] = n_re
            mm[r, pl.ds(wide + q * LANES, LANES)] = n_im
            new.extend((n_re, n_im))
        return tuple(new)

    lax.fori_loop(0, steps, state_rows, tuple(begin), unroll=2)

    mix_spread.pass_on()

    def read_rows(r):
        first, rest = split_two(mm[r, :])
        total = nt(first, out_blocks[...])
        total = total[:, :LANES] + total[:, LANES:] + nt(rest, out_blocks[pl.ds(0, LANES), :])
        drvp[r, :] = jax.nn.gelu(total + skip_row * drvp[r, :])

    blocks(read_rows)

    def back_rows(j, carry):
        r = pl.ds(pl.multiple_of(j * 8, 8), 8)
        drv[pl.ds(j, CHUNKS, stride=steps), :] = drvp[r, :]
        return carry

    lax.fori_loop(0, steps, back_rows, 0, unroll=8)
    state_all[:, pl.ds(lane_x, LANES)] = drv[...].astype(BF16)

    state_spread = Spread(state_all)
    state_spread.begin()

    arrive(st_all.at[pl.ds(0, cols - 1)], st_in)
    channels = cols * LANES
    mean = sum(st_all[k, 0:1, :] for k in range(cols)) * (1.0 / channels)
    square = sum(st_all[k, 1:2, :] for k in range(cols)) * (1.0 / channels)
    inv = lax.rsqrt(square - mean * mean + 1e-05)
    table = jnp.where(row_st == 0, inv, 0.0)
    for k in range(cols):
        offset = (st_all[k, 0:1, :] * (1.0 / LANES) - mean) * inv
        table = jnp.where(row_st == 1 + k, offset, table)
    st_rows[...] = table
    pick = ids((8, LANES), 0)

    def apply_norm(col):
        lanes = pl.ds(pl.multiple_of(col * LANES, LANES), LANES)
        scale = tn(st_rows[...], (pick == 0).astype(F32), HIGHEST)
        offset = tn(st_rows[...], (pick == 1 + col).astype(F32), HIGHEST)
        value = mix_all[:, lanes].astype(F32) * scale + offset
        value = value * st_all[col, 2:3, 0:LANES]
        conv_all[:, lanes] = (value * jax.nn.sigmoid(value)).astype(BF16)

    apply_norm(x)

    for k in reversed(far_first(side)):
        block = gp.at[c, turn(a_me, side - k)]
        arrive(block, p2_from[k - 1])
        send(block, block, pc_sem, pc_all, mate, x)

    mix_spread.finish()

    state_spread.pass_on()

    for k in range(1, cols):
        apply_norm(lax.rem(x + k, cols))

    arrive(gp.at[1 - c], pc_all)

    def place_out(line_y, carry):
        for plane_z in range(side):
            plane, col = divmod((plane_z + side - shift) % side, cols)
            for core in range(2):
                r = pl.ds(pl.multiple_of((plane * side + line_y) * 32 + core * 16, 16), 16)
                piece = gp[1, line_y, plane_z] if core else gp[0, plane_z, line_y]
                wo_conv[r, pl.ds(col * LANES, LANES)] = piece[:, :LANES]
                wo_state[r, pl.ds(col * LANES, LANES)] = piece[:, LANES:]
        return carry

    lax.fori_loop(0, side, place_out, 0)

    def early_rows(r):
        acc[r, :] = nt(conv_all[r, :], wo_conv[...])

    blocks(early_rows)

    state_spread.finish()

    def late_rows(r):
        out_ref[r, :] = (acc[r, :] + nt(state_all[r, :], wo_state[...])).astype(BF16)

    blocks(late_rows)

    for total, sem in outgoing:
        copy(total, total, sem, sem, mate, x).wait_send()
    for k in range(1, side):

        @pl.when(z + k < side)
        def _():
            block = mz_all.at[pl.ds(slot_z, 12), :]
            copy(block, block, cz_sems[k - 1], cz_sems[k - 1], mate, x).wait_send()

    assert next(free, None) is None


def sem_count(side, cols):
    operands, groups = 17, 16
    return operands + groups + 5 * (side - 1) + 3 + 4 + 3 + 1 + 2 * (6 if cols > 2 else 2)


def on_device(
    side,
    cols,
    tokens,
    norm_gain,
    w_value,
    w_gate,
    w_drive,
    conv_taps,
    conv_gain,
    log_step,
    step_shift,
    state_real,
    state_imag,
    in_map,
    out_map,
    skip_gain,
    start_state,
    conv_proj,
    state_proj,
):
    rows, depth = tokens.shape
    planes = side // cols
    out_cols = planes * side * 32
    groups, states = state_real.shape
    width = groups * states
    hbm = pl.BlockSpec(memory_space=pl.ANY)
    vmem = pl.BlockSpec(memory_space=pltpu.VMEM)
    small = (
        norm_gain.reshape(1, depth),
        conv_taps,
        conv_gain.reshape(1, -1),
        log_step.reshape(1, -1),
        step_shift.T,
        state_real,
        state_imag,
        jnp.transpose(in_map, (0, 1, 3, 2)).reshape(-1, states),
        out_map.reshape(-1, states),
        skip_gain,
        start_state.reshape(-1, states),
    )
    return pl.pallas_call(
        functools.partial(kernel, (side, cols)),
        out_shape=pltpu.VMEM((rows, out_cols), BF16),
        in_specs=[hbm] * 17,
        out_specs=vmem,
        scratch_shapes=[
            *[pltpu.VMEM(a.shape, F32) for a in small],
            pltpu.VMEM((rows, depth), BF16),
            pltpu.VMEM((rows, depth), BF16),
            pltpu.VMEM((2, side, side, 16, LANES), BF16),
            pltpu.VMEM((2, side, side, 16, 2 * LANES), BF16),
            pltpu.VMEM((16, 2 * LANES), BF16),
            pltpu.VMEM((2, side, side, 16, 2 * LANES), BF16),
            pltpu.VMEM((depth, LANES), BF16),
            pltpu.VMEM((depth, 2 * LANES), BF16),
            pltpu.VMEM((out_cols, cols * LANES), BF16),
            pltpu.VMEM((out_cols, cols * LANES), BF16),
            pltpu.VMEM((4, rows, LANES), F32),
            *[pltpu.VMEM((rows, width), F32)] * 4,
            pltpu.VMEM((rows, 2 * width), F32),
            pltpu.VMEM((2, 2 * LANES, width), BF16),
            pltpu.VMEM((2 * LANES, 2 * width), BF16),
            pltpu.VMEM((rows, LANES), F32),
            pltpu.VMEM((rows, LANES), F32),
            pltpu.VMEM((rows + 32, LANES), F32),
            pltpu.VMEM((rows, LANES), F32),
            pltpu.VMEM((32, LANES), BF16),
            pltpu.VMEM((32, LANES), BF16),
            pltpu.VMEM((cols, 8, rows), F32),
            pltpu.VMEM((8, rows), F32),
            pltpu.VMEM((16, LANES), F32),
            pltpu.VMEM((16, LANES), F32),
            pltpu.VMEM((side * 16, LANES), F32),
            pltpu.VMEM((side * 16, LANES), F32),
            *[pltpu.VMEM((rows, cols * LANES), BF16)] * 3,
            pltpu.VMEM((rows, out_cols), F32),
            pltpu.SemaphoreType.DMA((sem_count(side, cols),)),
        ],
        compiler_params=pltpu.CompilerParams(
            collective_id=0, has_side_effects=True, vmem_limit_bytes=60 * 1024 * 1024
        ),
    )(
        tokens,
        w_value,
        w_gate,
        w_drive,
        conv_proj.T,
        state_proj.T,
        *small,
    )


def solution(mesh):
    side = math.isqrt(mesh.shape["sp"] // 2)
    placed = (
        P("sp", None),
        P(),
        P("sp", "tp"),
        P("sp", "tp"),
        P("sp", "tp"),
        P(None, "tp"),
        P("tp"),
        P("tp"),
        P("sp", "tp"),
        P("tp", None),
        P("tp", None),
        P(None, "tp", None, None),
        P(None, "tp", None, None),
        P("tp", None),
        P(None, "tp", None),
        P("tp", "sp"),
        P("tp", "sp"),
    )
    return jax.shard_map(
        functools.partial(on_device, side, mesh.shape["tp"]),
        mesh=mesh,
        in_specs=placed,
        out_specs=P("sp", "tp"),
        check_vma=False,
    )
```
